32 devices in a mesh: sp: 8 (over z, y), tp: 4 (over x, core).
Axes of the slice: x: 2, y: 2, z: 4, core: 2. Of those that a mesh axis runs over, the one named last changes fastest.
Arguments:
- stream: bfloat16 [3072, 2048], P(('sp', 'tp')), may hold values from -6 to 6
- query_nope: bfloat16 [3072, 16, 128], P('sp', 'tp'), may hold values from -6 to 6
- query_rope: bfloat16 [3072, 16, 64], P('sp', 'tp'), may hold values from -700 to 700
- latent: bfloat16 [3072, 512], P('sp'), may hold values from -6 to 6
- rope_key: bfloat16 [3072, 64], P('sp'), may hold values from -6 to 6
- latent_gain: float32 [512], replicated, may hold values from 0.1 to 1.9
- key_up: bfloat16 [512, 16, 128], P(None, 'tp'), may hold values from -0.375 to 0.375
- value_up: bfloat16 [512, 16, 128], P(None, 'tp'), may hold values from -2.6516504 to 2.6516504
- out_gain: float32 [2048], P('tp'), may hold values from 0.1 to 1.9
- out_weight: bfloat16 [2048, 2048], P('tp'), may hold values from -0.125 to 0.125
- norm_gain: float32 [2048], replicated, may hold values from 0.1 to 1.9
- ff_in: bfloat16 [2048, 8192], P('sp', 'tp'), may hold values from -0.125 to 0.125
- ff_out: bfloat16 [8192, 2048], P('tp', 'sp'), may hold values from -0.0625 to 0.0625
Outputs:
- layer_out: bfloat16 [3072, 2048], P(('sp', 'tp'))
The draws below stay inside these ranges and needn't reach their ends.
All inputs are finite; a program needn't handle non-finite values.
Results may differ from the reference program's by a relative error of at most 0.018.
Values may be sent and summed in bfloat16 or wider, within the bound.
A program may use at most 128 MiB of HBM per device.

```python
import math
import jax
import jax.numpy as jnp
from jax import lax

D = 2048
FF = 8192
HEADS = 16
NOPE = 128
ROPE = 64
LATENT = 512
VDIM = 128
TOKENS = 3072


def draw_query_rope(key, part):
    base_draw = jax.random.normal(key, (TOKENS, HEADS, ROPE), jnp.float32)
    return jnp.clip(base_draw, -700.0, 700.0).astype(jnp.bfloat16)


def draw_value_up(key, part):
    base_draw = jnp.clip(jax.random.normal(key, (LATENT, HEADS, VDIM), jnp.float32), -6.0, 6.0) / jnp.sqrt(jnp.float32(LATENT))
    factor = jnp.power(4.0, jnp.arange(HEADS, dtype=jnp.float32) / max(HEADS - 1, 1))
    return (base_draw * factor[None, :, None]).astype(jnp.bfloat16)


def block_levels(rng, extent, split, low, largest):
    def one(axis_at, blocks):
        heights = jax.random.uniform(jax.random.fold_in(jax.random.fold_in(rng, 6), axis_at), (blocks,), jnp.float32, low / len(split), largest / len(split))
        return jnp.repeat(jnp.exp(heights), extent[axis_at] // blocks).reshape((-1,) + (1,) * (len(extent) - axis_at - 1))

    level = one(*split[0])
    for cut in split[1:]:
        level = level * one(*cut)
    return level


def scatter_about(key, shape, scale, reach, split=(), kind=jnp.bfloat16):
    entries = scale * jax.random.normal(key, shape, jnp.float32)
    if split:
        entries = entries * block_levels(key, shape, split, -0.22, 0.18)
    return jnp.clip(entries, -reach, reach).astype(kind)


def setup_inputs(seed: int = 0) -> dict:
    key_list = jax.random.split(jax.random.key(seed), 14)
    stream = scatter_about(key_list[0], (TOKENS, D), 1.0, 6.0, ((0, 32),))
    query_nope = scatter_about(key_list[1], (TOKENS, HEADS, NOPE), 1.0, 6.0, ((0, 8), (1, 4)))
    query_rope = draw_query_rope(jax.random.fold_in(key_list[13], 71), 0)
    latent = scatter_about(key_list[3], (TOKENS, LATENT), 1.0, 6.0, ((0, 8),))
    rope_key = scatter_about(key_list[4], (TOKENS, ROPE), 1.0, 6.0, ((0, 8),))
    latent_gain = jnp.clip(1.0 + 0.18 * jax.random.normal(key_list[5], (LATENT,), jnp.float32), 0.1, 1.9)
    key_up = scatter_about(key_list[6], (LATENT, HEADS, NOPE), (2 * NOPE) ** -0.5, 0.375, ((1, 4),))
    value_up = draw_value_up(jax.random.fold_in(key_list[13], 71), 0)
    out_gain = jnp.clip(1.0 + 0.18 * jax.random.normal(key_list[8], (HEADS * VDIM,), jnp.float32), 0.1, 1.9)
    out_weight = scatter_about(key_list[9], (HEADS * VDIM, D), (HEADS * VDIM) ** -0.5, 0.125, ((0, 4),))
    norm_gain = jnp.clip(1.0 + 0.18 * jax.random.normal(key_list[10], (D,), jnp.float32), 0.1, 1.9)
    ff_in = scatter_about(key_list[11], (D, FF), D ** -0.5, 0.125, ((0, 8), (1, 4)))
    ff_out = scatter_about(key_list[12], (FF, D), FF ** -0.5, 0.0625, ((0, 4), (1, 8)))
    return {"stream": stream, "query_nope": query_nope, "query_rope": query_rope, "latent": latent, "rope_key": rope_key, "latent_gain": latent_gain, "key_up": key_up, "value_up": value_up, "out_gain": out_gain, "out_weight": out_weight, "norm_gain": norm_gain, "ff_in": ff_in, "ff_out": ff_out}


EPS = 1e-06
THETA = 10000.0

def turn(values, positions):
    full_width = values.shape[-1]
    half_width = full_width // 2
    inverse = jnp.power(THETA, -jnp.arange(0, full_width, 2, dtype=jnp.float32) / full_width)
    angles = positions[:, None] * inverse[None, :]
    cosine = jnp.cos(angles)
    sine_part = jnp.sin(angles)
    if values.ndim == 3:
        cosine = cosine[:, None, :]
        sine_part = sine_part[:, None, :]
    vector = values.astype(jnp.float32)
    lower_half = vector[..., :half_width]
    upper_half = vector[..., half_width:]
    return jnp.concatenate([lower_half * cosine - upper_half * sine_part, lower_half * sine_part + upper_half * cosine], axis=-1)

def reference(stream, query_nope, query_rope, latent, rope_key, latent_gain, key_up, value_up, out_gain, out_weight, norm_gain, ff_in, ff_out):
    positions = jnp.arange(TOKENS, dtype=jnp.float32)
    lat_full = latent.astype(jnp.float32)
    normed = (lat_full * lax.rsqrt(lax.optimization_barrier(jnp.mean(lat_full * lat_full, axis=-1, keepdims=True)) + EPS) * latent_gain.astype(jnp.float32)).astype(jnp.bfloat16)
    keys_rot = turn(rope_key, positions).astype(jnp.bfloat16)
    query_rot = turn(query_rope, positions).astype(jnp.bfloat16)
    query_lat = jnp.einsum('thn,lhn->thl', query_nope.astype(jnp.float32), key_up.astype(jnp.float32)).astype(jnp.bfloat16)
    score_scale = 1.0 / math.sqrt(NOPE + ROPE)
    normed_wide = normed.astype(jnp.float32)
    keys_wide = keys_rot.astype(jnp.float32)

    def attend(inputs):
        lat_query, rot_query = inputs
        scores = (jnp.einsum('thl,kl->thk', lat_query.astype(jnp.float32), normed_wide) + jnp.einsum('thr,kr->thk', rot_query.astype(jnp.float32), keys_wide)) * score_scale
        row_max = lax.optimization_barrier(jnp.max(scores, axis=-1, keepdims=True))
        expo = jnp.exp(scores - row_max)
        denom = lax.optimization_barrier(jnp.sum(expo, axis=-1))
        probs = lax.optimization_barrier(expo.astype(jnp.bfloat16)).astype(jnp.float32)
        summed = jnp.einsum('thk,kl->thl', probs, normed_wide)
        return (summed / denom[..., None]).astype(jnp.bfloat16)
    q_block = math.gcd(TOKENS, 512)
    out_lat = lax.map(attend, (query_lat.reshape(TOKENS // q_block, q_block, HEADS, LATENT), query_rot.reshape(TOKENS // q_block, q_block, HEADS, ROPE)))
    out_lat = out_lat.reshape(TOKENS, HEADS, LATENT)
    head_out = jnp.einsum('thl,lhv->thv', out_lat.astype(jnp.float32), value_up.astype(jnp.float32))
    row_scale = lax.rsqrt(lax.optimization_barrier(jnp.mean(head_out * head_out, axis=(1, 2))) + EPS)
    gated = (head_out.reshape(TOKENS, HEADS * VDIM) * out_gain.astype(jnp.float32)).astype(jnp.bfloat16)
    mid_stream = stream.astype(jnp.float32) + row_scale[:, None] * jnp.dot(gated, out_weight, preferred_element_type=jnp.float32)
    ff_input = (mid_stream * lax.rsqrt(lax.optimization_barrier(jnp.mean(mid_stream * mid_stream, axis=-1, keepdims=True)) + EPS) * norm_gain.astype(jnp.float32)).astype(jnp.bfloat16)
    pre_act = jnp.dot(ff_input, ff_in, preferred_element_type=jnp.float32)
    activation = jnp.square(jax.nn.relu(pre_act)).astype(jnp.bfloat16)
    return (mid_stream + jnp.dot(activation, ff_out, preferred_element_type=jnp.float32)).astype(jnp.bfloat16)
```

```python
import functools
import math

import jax
import jax.numpy as jnp
from jax import lax
from jax.experimental import pallas as pl
from jax.experimental.pallas import tpu as pltpu
from jax.sharding import PartitionSpec as P

EPS = 1e-06
THETA = 10000.0
F32 = jnp.float32
BF16 = jnp.bfloat16
MESH = pl.DeviceIdType.MESH
LANES = 128


def turn(values, positions):
    full_width = values.shape[-1]
    half_width = full_width // 2
    inverse = jnp.power(THETA, -jnp.arange(0, full_width, 2, dtype=F32) / full_width)
    angles = positions[:, None] * inverse[None, :]
    cosine = jnp.cos(angles)
    sine_part = jnp.sin(angles)
    if values.ndim == 3:
        cosine = cosine[:, None, :]
        sine_part = sine_part[:, None, :]
    vector = values.astype(F32)
    lower_half = vector[..., :half_width]
    upper_half = vector[..., half_width:]
    return jnp.concatenate(
        [
            lower_half * cosine - upper_half * sine_part,
            lower_half * sine_part + upper_half * cosine,
        ],
        axis=-1,
    )


def ring_shape(n):
    rows = 1
    while rows * rows < n:
        rows *= 2
    return (rows, n // rows) if n % rows == 0 else (n, 1)


def ring_pos(nz, ny, index):
    if ny == 1:
        return index
    z, y = lax.div(index, ny), lax.rem(index, ny)
    r = nz - 1 - z
    odd = lax.rem(r, 2)
    c = (1 - odd) * (y - 1) + odd * (ny - 1 - y)
    return jnp.where(y == 0, z, nz + r * (ny - 1) + c)


def ring_at(nz, ny, pos):
    if ny == 1:
        return pos
    q = jnp.maximum(pos - nz, 0)
    r, c = lax.div(q, ny - 1), lax.rem(q, ny - 1)
    odd = lax.rem(r, 2)
    y = 1 + (1 - odd) * c + odd * (ny - 2 - c)
    return jnp.where(pos < nz, pos * ny, (nz - 1 - r) * ny + y)


def flip(index, bits):
    bit = 1
    out = index
    while bit <= bits:
        if bits & bit:
            out = out + bit * (1 - 2 * lax.rem(lax.div(index, bit), 2))
        bit *= 2
    return out


def kernel(
    n, tp, heads, latent_width, width,
    kv_ref, q_ref, vup_ref, gain_ref, ow_ref, stream_ref, ngain_ref, ffin_ref, ffout_ref,
    out_ref,
    kv, fi, fo, ow, sc, top, acc, gated, pout, pin, keep, xout, xin, sq_out, sq_in, mid, xs, act,
    fresh, mixed, mpo, mpi, mxo, mxi, mzo, mzi,
    local_sem, ka_send, ka_recv, kx_send, kx_recv, kp_send, kp_recv,
    c_send, c_recv, w_send, w_recv,
    s_send, s_recv, r_send, r_recv, g_send, g_recv,
    mp_send, mp_recv, mx_send, mx_recv, mz_send, mz_recv,
):
    sp = lax.axis_index("sp")
    me = lax.axis_index("tp")
    nz, ny = ring_shape(n)
    hz, m, nx = nz // 2, n // 2, tp // 2
    z, y = lax.div(sp, ny), lax.rem(sp, ny)
    x, core = lax.div(me, 2), lax.rem(me, 2)
    half, local = lax.div(sp, m), lax.rem(sp, m)
    zl = lax.div(local, ny)
    mate = lax.rem(sp + m, n)
    pcore = me + 1 - 2 * core
    rows = q_ref.shape[1]
    share = rows // tp
    dblk = width // n
    hh = act.shape[2]
    chunk = sc.shape[3]
    vdim = LANES
    pos = ring_pos(hz, ny, local)

    def at(offset):
        return half * m + ring_at(hz, ny, lax.rem(pos + offset + m, m))

    turnway = lax.rem(pos, 2)

    def space(kz, ky):
        return flip(z, kz) * ny + flip(y, ky)

    def along(kx, c):
        return flip(x, kx) * 2 + c

    sends = []

    def remote(a, b, s, r, to, when=None):
        cp = pltpu.make_async_remote_copy(a, b, s, r, device_id=to, device_id_type=MESH)
        cp.start()
        sends.append(cp)

    def arrived(ref, s, r):
        pltpu.make_async_remote_copy(
            ref, ref, s, r, device_id=(sp, pcore), device_id_type=MESH).wait_recv()

    def lanes(h):
        return pl.ds(pl.multiple_of(h * hh, LANES), hh)

    def deep(h):
        return pl.ds(pl.multiple_of(h * hh, LANES), hh)

    def block_rows(s):
        return pl.ds(pl.multiple_of(s * dblk, dblk), dblk)

    own = [
        pltpu.make_async_copy(kv_ref, kv.at[pl.ds(sp * rows, rows)], local_sem.at[0]),
        pltpu.make_async_copy(ffin_ref.at[:, lanes(half)], fi.at[block_rows(sp)], local_sem.at[1]),
        pltpu.make_async_copy(ffout_ref.at[deep(half)], fo.at[sp], local_sem.at[2]),
        pltpu.make_async_copy(ow_ref, ow, local_sem.at[3]),
    ]
    for cp in own:
        cp.start()

    barrier = pltpu.get_barrier_semaphore()
    for i in range(1, n):
        pl.semaphore_signal(
            barrier, inc=1, device_id=(lax.rem(sp + i, n), me), device_id_type=MESH)
    for j in range(1, tp):
        pl.semaphore_signal(
            barrier, inc=1, device_id=(sp, lax.rem(me + j, tp)), device_id_type=MESH)
    pl.semaphore_wait(barrier, n + tp - 2)

    def piece(s, t):
        return kv.at[pl.ds(pl.multiple_of(s * rows + t * share, share), share)]

    def arrive(kz, ky):
        ref = piece(space(kz, ky), me)
        i = kz * ny + ky
        arrived(ref, ka_send.at[i], ka_recv.at[i])
        if ky == 0:
            for k in range(1, ny):
                j = kz * ny + k
                remote(ref, ref, ka_send.at[j], ka_recv.at[j], (space(0, k), me))
        for kx in range(1, nx):
            remote(ref, ref, kx_send.at[i, kx], kx_recv.at[i, kx], (sp, along(kx, core)))
        remote(ref, ref, kp_send.at[i, 0], kp_recv.at[i, 0], (sp, pcore))

    def across(kz, ky):
        i = kz * ny + ky
        for kx in range(1, nx):
            ref = piece(space(kz, ky), along(kx, core))
            arrived(ref, kx_send.at[i, kx], kx_recv.at[i, kx])
            remote(ref, ref, kp_send.at[i, kx], kp_recv.at[i, kx], (sp, pcore))

    def settle(kz, ky):
        i = kz * ny + ky
        for kx in range(nx):
            ref = piece(space(kz, ky), along(kx, 1 - core))
            arrived(ref, kp_send.at[i, kx], kp_recv.at[i, kx])

    def inner_of(h):
        return (hz - 1) * (1 - h)

    def is_inner(hm):
        return lax.div(lax.rem(hm, m), ny) == inner_of(half)

    def w_whole(b, s):
        return fi.at[block_rows(s)] if b == 0 else fo.at[s]

    def w_ref(b, s, way):
        if b == 0:
            return fi.at[pl.ds(pl.multiple_of(s * dblk + way * (dblk // 2), dblk // 2), dblk // 2)]
        return fo.at[s, pl.ds(pl.multiple_of(way * (hh // 2), hh // 2), hh // 2)]

    def home(way, step):
        return at((2 * way - 1) * step)

    def source(g, hm):
        if g == 0:
            return hm
        return (1 - half) * m + (g - 1) * ny + lax.rem(hm, ny)

    def cross(b):
        to = (1 - half) * m + inner_of(1 - half) * ny + y
        a = ffin_ref.at[:, lanes(1 - half)] if b == 0 else ffout_ref.at[deep(1 - half)]
        remote(a, w_whole(b, sp), c_send.at[b], c_recv.at[b, zl], (to, me))

    guarded = []

    def unit(b, g, step, k):
        way = turnway if k == 0 else 1 - turnway
        hm = home(way, step)
        s = source(g, hm)
        ref = w_ref(b, s, way)
        cp = pltpu.make_async_remote_copy(
            ref, ref, w_send.at[b, g, way, step], w_recv.at[b, g, way, step],
            device_id=(at(1 - 2 * way), me), device_id_type=MESH)

        def go():
            if step > 0:
                arrived(ref, w_send.at[b, g, way, step - 1], w_recv.at[b, g, way, step - 1])
            elif g > 0 and k == 0:
                arrived(w_whole(b, s), c_send.at[b], c_recv.at[b, g - 1])
            if step < m - 1:
                cp.start()

        if g == 0:
            go()
            if step < m - 1:
                sends.append(cp)
        else:
            pl.when(is_inner(hm))(go)
            if step < m - 1:
                guarded.append((hm, cp))

    others = range(1, hz + 1)
    issued = set()

    def do(b, g, step, k):
        if step < m and (b, g, step, k) not in issued:
            if step > 0:
                do(b, g, step - 1, k)
            issued.add((b, g, step, k))
            unit(b, g, step, k)

    def near(b, step, *ks):
        for k in ks:
            do(b, 0, step, k)

    def far(b, step, *ks):
        for k in ks:
            for g in others:
                do(b, g, step, k)

    own[0].wait()
    mine = piece(sp, me)
    for ky in range(1, ny):
        remote(mine, mine, ka_send.at[ky], ka_recv.at[ky], (space(0, ky), me))
    for kz in range(1, nz):
        remote(mine, mine, ka_send.at[kz * ny], ka_recv.at[kz * ny], (space(kz, 0), me))
    own[1].wait()
    near(0, 0, 0, 1)

    scale = 1.0 / math.sqrt(LANES + (q_ref.shape[2] - latent_width) // 2)

    def score(kz):
        keys = pl.ds(pl.multiple_of(flip(z, kz) * chunk, chunk), chunk)

        def one(h, _):
            s = lax.dot_general(
                q_ref[h], kv[keys, :], (((1,), (1,)), ((), ())),
                preferred_element_type=F32) * scale
            sc[kz, h] = s
            best = jnp.max(s, axis=1, keepdims=True)
            if kz > 0:
                best = jnp.maximum(best, top[h][:, :1])
            top[h] = jnp.broadcast_to(best, (rows, LANES))
            return 0

        lax.fori_loop(0, heads, one, 0)

    for ky in range(1, ny):
        arrive(0, ky)
    arrive(1, 0)
    for ky in range(1, ny):
        across(0, ky)
    for kz in range(2, nz):
        arrive(kz, 0)
    own[2].wait()
    cross(0)
    near(1, 0, 0, 1)
    for ky in range(1, ny):
        settle(0, ky)
    for ky in range(1, ny):
        arrive(1, ky)
    score(0)
    for kz in range(1, nz):
        for ky in range(1, ny):
            if kz > 1:
                arrive(kz, ky)
    near(0, 1, 0)
    for kz in range(1, nz):
        for ky in range(ny):
            across(kz, ky)
        for ky in range(ny):
            settle(kz, ky)
        score(kz)
        if kz == 1:
            cross(1)
            near(1, 1, 0)
            near(0, 1, 1)
        elif kz == nz - 1:
            far(0, 0, 0, 1)

    squares = jnp.zeros((rows, 1), F32)
    for h in range(heads):
        peak = top[h][:, :1]
        acc[...] = jnp.zeros_like(acc)

        def gather(kz, den):
            zk = flip(z, 0)
            zk = jnp.where(kz == 0, z, zk)
            for k in range(1, nz):
                zk = jnp.where(kz == k, flip(z, k), zk)
            e = jnp.exp(sc[kz, h] - peak)
            acc[...] += jnp.dot(
                e.astype(BF16),
                kv[pl.ds(pl.multiple_of(zk * chunk, chunk), chunk), pl.ds(0, latent_width)],
                preferred_element_type=F32)
            return den + jnp.sum(e, axis=1, keepdims=True)

        den = lax.fori_loop(0, nz, gather, jnp.zeros((rows, 1), F32))
        lat = (acc[...] / den).astype(BF16)
        cols = slice(h * vdim, (h + 1) * vdim)
        one = jnp.dot(lat, vup_ref[:, cols], preferred_element_type=F32)
        squares = squares + jnp.sum(one * one, axis=1, keepdims=True)
        scaled = (one * gain_ref[:, cols]).astype(BF16)
        for t in range(tp):
            gated[t % 2, (t // 2) * share:(t // 2 + 1) * share, cols] = (
                scaled[t * share:(t + 1) * share])
        if h == 0:
            near(0, 2, 0)
            near(1, 1, 1)
        elif h == heads // 2:
            near(0, 2, 1)
    sq_out[...] = jnp.broadcast_to(squares, sq_out.shape)
    own[3].wait()

    tile = width // 4

    def project(which, put):
        def one(c, _):
            cols = pl.ds(pl.multiple_of(c * tile, tile), tile)
            got = jnp.dot(gated[which], ow[:, cols], preferred_element_type=F32)
            put(cols, got.reshape(nx, share, tile))
            return 0
        lax.fori_loop(0, 4, one, 0)

    def put_out(cols, got):
        pout[:, :, cols] = got.astype(BF16)

    def put_keep(cols, got):
        keep[:, :, cols] = got

    project(1 - core, put_out)
    remote(pout, pin, r_send.at[0], r_recv.at[0], (sp, pcore))
    for j in range(1, tp):
        to = lax.rem(me + j, tp)
        remote(sq_out.at[pl.ds(pl.multiple_of(to * share, share), share)], sq_in.at[j],
               s_send.at[j], s_recv.at[j], (sp, to))
    project(core, put_keep)
    arrived(pin, r_send.at[0], r_recv.at[0])
    for kx in range(1, nx):
        xi = flip(x, kx)
        xout[kx] = (keep[xi] + pin[xi].astype(F32)).astype(BF16)
        remote(xout.at[kx], xin.at[kx], r_send.at[kx], r_recv.at[kx], (sp, along(kx, core)))
    far(0, 1, 0, 1)
    near(1, 2, 0)
    far(1, 0, 0, 1)
    near(1, 2, 1)
    summed = keep[x] + pin[x].astype(F32)
    square = sq_out[pl.ds(pl.multiple_of(me * share, share), share)]
    for j in range(1, tp):
        arrived(sq_in.at[j], s_send.at[j], s_recv.at[j])
        square = square + sq_in[j]
    for kx in range(1, nx):
        arrived(xin.at[kx], r_send.at[kx], r_recv.at[kx])
        summed = summed + xin[kx].astype(F32)
    row_scale = lax.rsqrt(square[:, :1] / (heads * tp * vdim) + EPS)
    middle = stream_ref[...].astype(F32) + row_scale * summed
    mid[...] = middle
    norm = lax.rsqrt(jnp.mean(middle * middle, axis=1, keepdims=True) + EPS)

    def seat(kx, c):
        return c * nx + flip(x, kx)

    xs[0, seat(0, core)] = (middle * norm * ngain_ref[...]).astype(BF16)

    def hand(s, kx):
        ref = xs.at[s, seat(kx, core)]
        remote(ref, ref, g_send.at[1, s, kx], g_recv.at[1, s, kx], (sp, pcore))

    def spread(s):
        ref = xs.at[s, seat(0, core)]
        for kx in range(1, nx):
            remote(ref, ref, g_send.at[0, s, kx], g_recv.at[0, s, kx], (sp, along(kx, core)))
        hand(s, 0)

    def collect(s):
        for kx in range(1, nx):
            arrived(xs.at[s, seat(kx, core)], g_send.at[0, s, kx], g_recv.at[0, s, kx])
            hand(s, kx)

    def settled(s):
        for kx in range(nx):
            arrived(xs.at[s, seat(kx, 1 - core)], g_send.at[1, s, kx], g_recv.at[1, s, kx])

    ref = xs.at[0, seat(0, core)]
    remote(ref, xs.at[1, seat(0, core)], g_send.at[0, 0, 0], g_recv.at[0, 0, 0], (mate, me))
    spread(0)
    far(0, 2, 0, 1)
    near(0, m - 1, 0, 1)
    collect(0)
    settled(0)
    far(1, 1, 0)
    far(0, m - 1, 0, 1)

    wide = 512 if hh % 512 == 0 else 128

    def first(s):
        for c in range(hh // wide):
            cols = slice(c * wide, (c + 1) * wide)
            pre = jnp.dot(
                xs[s].reshape(rows, width), fi[:, cols], preferred_element_type=F32)
            pre = jnp.maximum(pre, 0.0)
            act[s, :, cols] = (pre * pre).astype(BF16)

    flow = []
    for k in range(m):
        flow.append((0, at(k)))
    for g in others:
        for ky in range(ny):
            flow.append((g, (1 - half) * m + (g - 1) * ny + flip(y, ky)))

    def stage_dot(i, u):
        got = jnp.dot(act[u], fo[flow[i][1]], preferred_element_type=F32)
        fresh[...] = got.reshape(2, nx, share, dblk)
        mixed[i, u] = fresh[core]
        mpo[i, u] = fresh[1 - core].astype(BF16)
        remote(mpo.at[i, u], mpi.at[i, u], mp_send.at[i, u], mp_recv.at[i, u], (sp, pcore))

    def stage_core(i, u):
        arrived(mpi.at[i, u], mp_send.at[i, u], mp_recv.at[i, u])
        for kx in range(1, nx):
            xi = flip(x, kx)
            mxo[i, u, kx] = (
                mixed[i, u, xi] + mpi[i, u, xi].astype(F32)).astype(BF16)
            remote(mxo.at[i, u, kx], mxi.at[i, u, kx], mx_send.at[i, u, kx],
                   mx_recv.at[i, u, kx], (sp, along(kx, core)))

    def stage_x(i, u):
        s = flow[i][1]
        v = mixed[i, u, x] + mpi[i, u, x].astype(F32)
        for kx in range(1, nx):
            arrived(mxi.at[i, u, kx], mx_send.at[i, u, kx], mx_recv.at[i, u, kx])
            v = v + mxi[i, u, kx].astype(F32)
        if u == 1:
            mzo[s] = v.astype(BF16)
            remote(mzo.at[s], mzi.at[s], mz_send.at[s], mz_recv.at[s], (mate, me))
        else:
            cols = pl.ds(pl.multiple_of(s * dblk, dblk), dblk)
            mid[:, cols] = mid[:, cols] + v

    to_core, to_x = [], []

    def drain(cores, xs_left):
        while len(to_core) > cores:
            stage_core(*to_core[0])
            to_x.append(to_core.pop(0))
        while len(to_x) > xs_left:
            stage_x(*to_x.pop(0))

    def push(i, u):
        stage_dot(i, u)
        to_core.append((i, u))
        drain(2, 4)

    arrived(xs.at[1, seat(0, core)], g_send.at[0, 0, 0], g_recv.at[0, 0, 0])
    spread(1)
    first(0)
    near(1, m - 1, 0, 1)
    for i in range(m):
        push(i, 0)
    drain(0, 8)
    far(1, 1, 1)
    collect(1)
    settled(1)
    first(1)
    far(1, 2, 1)
    for i in range(m):
        push(i, 1)
    far(1, 2, 0)
    far(1, m - 1, 0, 1)
    for i in range(m, n):
        push(i, 1)
    for i in range(m, n):
        push(i, 0)
    drain(0, 0)
    for i in range(n):
        s = flow[i][1]
        arrived(mzi.at[s], mz_send.at[s], mz_recv.at[s])
        cols = pl.ds(pl.multiple_of(s * dblk, dblk), dblk)
        out_ref[:, cols] = (mid[:, cols] + mzi[s].astype(F32)).astype(BF16)

    for cp in sends:
        cp.wait_send()
    for hm, cp in guarded:
        pl.when(is_inner(hm))(cp.wait_send)


def body(
    n, tp,
    stream, query_nope, query_rope, latent, rope_key, latent_gain,
    key_up, value_up, out_gain, out_weight, norm_gain, ff_in, ff_out,
):
    rows, heads = query_nope.shape[:2]
    width = stream.shape[1]
    latent_width = latent.shape[1]
    rope = rope_key.shape[1]
    pad = -rope % LANES
    dblk, hidden = ff_in.shape
    share = rows // tp
    positions = (lax.axis_index("sp") * rows + jnp.arange(rows, dtype=jnp.int32)).astype(F32)
    lat_full = latent.astype(F32)
    normed = (
        lat_full
        * lax.rsqrt(jnp.mean(lat_full * lat_full, axis=-1, keepdims=True) + EPS)
        * latent_gain
    ).astype(BF16)
    keys_rot = turn(rope_key, positions).astype(BF16)
    query_rot = turn(query_rope, positions).astype(BF16)
    query_lat = jnp.einsum(
        "thn,lhn->htl", query_nope, key_up, preferred_element_type=F32
    ).astype(BF16)
    kv = jnp.concatenate([normed, keys_rot, jnp.zeros((rows, pad), BF16)], axis=1)
    q = jnp.concatenate(
        [query_lat, query_rot.transpose(1, 0, 2), jnp.zeros((heads, rows, pad), BF16)], axis=2
    )
    keys = n * rows
    nz, ny = ring_shape(n)
    hz, m, nx = nz // 2, n // 2, tp // 2
    chunk = ny * rows
    hh = hidden // 2
    wide = kv.shape[1]
    vm = pl.BlockSpec(memory_space=pltpu.VMEM)
    hbm = pl.BlockSpec(memory_space=pl.ANY)
    dma = pltpu.SemaphoreType.DMA
    return pl.pallas_call(
        functools.partial(kernel, n, tp, heads, latent_width, width),
        out_shape=jax.ShapeDtypeStruct((share, width), BF16),
        in_specs=[hbm, vm, vm, vm, hbm, vm, vm, hbm, hbm],
        out_specs=vm,
        scratch_shapes=[
            pltpu.VMEM((keys, wide), BF16),
            pltpu.VMEM((width, hh), BF16),
            pltpu.VMEM((n, hh, dblk), BF16),
            pltpu.VMEM(out_weight.shape, BF16),
            pltpu.VMEM((nz, heads, rows, chunk), F32),
            pltpu.VMEM((heads, rows, LANES), F32),
            pltpu.VMEM((rows, latent_width), F32),
            pltpu.VMEM((2, nx * share, out_weight.shape[0]), BF16),
            pltpu.VMEM((nx, share, width), BF16),
            pltpu.VMEM((nx, share, width), BF16),
            pltpu.VMEM((nx, share, width), F32),
            pltpu.VMEM((nx, share, width), BF16),
            pltpu.VMEM((nx, share, width), BF16),
            pltpu.VMEM((rows, LANES), F32),
            pltpu.VMEM((tp, share, LANES), F32),
            pltpu.VMEM((share, width), F32),
            pltpu.VMEM((2, tp, share, width), BF16),
            pltpu.VMEM((2, rows, hh), BF16),
            pltpu.VMEM((2, nx, share, dblk), F32),
            pltpu.VMEM((n, 2, nx, share, dblk), F32),
            pltpu.VMEM((n, 2, nx, share, dblk), BF16),
            pltpu.VMEM((n, 2, nx, share, dblk), BF16),
            pltpu.VMEM((n, 2, nx, share, dblk), BF16),
            pltpu.VMEM((n, 2, nx, share, dblk), BF16),
            pltpu.VMEM((n, share, dblk), BF16),
            pltpu.VMEM((n, share, dblk), BF16),
            dma((4,)),
            dma((n,)), dma((n,)), dma((n, nx)), dma((n, nx)), dma((n, nx)), dma((n, nx)),
            dma((2,)), dma((2, hz)),
            dma((2, hz + 1, 2, m)), dma((2, hz + 1, 2, m)),
            dma((tp,)), dma((tp,)), dma((nx,)), dma((nx,)),
            dma((2, 2, nx)), dma((2, 2, nx)),
            dma((n, 2)), dma((n, 2)), dma((n, 2, nx)), dma((n, 2, nx)), dma((n,)), dma((n,)),
        ],
        compiler_params=pltpu.CompilerParams(
            collective_id=0, has_side_effects=True, vmem_limit_bytes=63 * 1024 * 1024
        ),
    )(
        kv, q, value_up.reshape(latent_width, -1), out_gain[None, :], out_weight,
        stream, norm_gain[None, :], ff_in, ff_out,
    )


def solution(mesh):
    placed = (
        P(("sp", "tp"), None),
        P("sp", "tp", None),
        P("sp", "tp", None),
        P("sp", None),
        P("sp", None),
        P(),
        P(None, "tp", None),
        P(None, "tp", None),
        P("tp"),
        P("tp", None),
        P(),
        P("sp", "tp"),
        P("tp", "sp"),
    )
    return jax.shard_map(
        functools.partial(body, mesh.shape["sp"], mesh.shape["tp"]),
        mesh=mesh, in_specs=placed, out_specs=P(("sp", "tp"), None), check_vma=False
    )
```

```python
import functools
import math

import jax
import jax.numpy as jnp
from jax import lax
from jax.experimental import pallas as pl
from jax.experimental.pallas import tpu as pltpu
from jax.sharding import PartitionSpec as P

EPS = 1e-06
THETA = 10000.0
F32 = jnp.float32
BF16 = jnp.bfloat16
MESH = pl.DeviceIdType.MESH
LANES = 128


def ring_shape(n):
    rows = 1
    while rows * rows < n:
        rows *= 2
    return (rows, n // rows) if n % rows == 0 else (n, 1)


def ring_pos(nz, ny, index):
    if ny == 1:
        return index
    z, y = lax.div(index, ny), lax.rem(index, ny)
    r = nz - 1 - z
    odd = lax.rem(r, 2)
    c = (1 - odd) * (y - 1) + odd * (ny - 1 - y)
    return jnp.where(y == 0, z, nz + r * (ny - 1) + c)


def ring_at(nz, ny, pos):
    if ny == 1:
        return pos
    q = jnp.maximum(pos - nz, 0)
    r, c = lax.div(q, ny - 1), lax.rem(q, ny - 1)
    odd = lax.rem(r, 2)
    y = 1 + (1 - odd) * c + odd * (ny - 2 - c)
    return jnp.where(pos < nz, pos * ny, (nz - 1 - r) * ny + y)


def flip(index, bits):
    bit = 1
    out = index
    while bit <= bits:
        if bits & bit:
            out = out + bit * (1 - 2 * lax.rem(lax.div(index, bit), 2))
        bit *= 2
    return out


def kernel(
    n, tp, heads, latent_width, width,
    lat_ref, lgain_ref, rk_ref, cos_ref, sin_ref, qn_ref, qr_ref, kup_ref, vup_ref,
    gain_ref, ow_ref, stream_ref, ngain_ref, ffin_ref, ffout_ref,
    out_ref,
    qraw, kraw, vraw, plain, q, vup, kv, fi, fo, ow, sc, top, acc, gated, pout, pin, keep, xout, xin, sq_out, sq_in, mid, xs, act,
    fresh, mixed, mpo, mpi, mxo, mxi, mzo, mzi,
    local_sem, ka_send, ka_recv, kx_send, kx_recv, kp_send, kp_recv,
    c_send, c_recv, w_send, w_recv,
    s_send, s_recv, r_send, r_recv, g_send, g_recv,
    mp_send, mp_recv, mx_send, mx_recv, mz_send, mz_recv,
):
    sp = lax.axis_index("sp")
    me = lax.axis_index("tp")
    nz, ny = ring_shape(n)
    hz, m, nx = nz // 2, n // 2, tp // 2
    z, y = lax.div(sp, ny), lax.rem(sp, ny)
    x, core = lax.div(me, 2), lax.rem(me, 2)
    half, local = lax.div(sp, m), lax.rem(sp, m)
    zl = lax.div(local, ny)
    mate = lax.rem(sp + m, n)
    pcore = me + 1 - 2 * core
    rows = q.shape[1]
    share = rows // tp
    dblk = width // n
    hh = act.shape[2]
    chunk = sc.shape[3]
    vdim = LANES
    pos = ring_pos(hz, ny, local)

    def at(offset):
        return half * m + ring_at(hz, ny, lax.rem(pos + offset + m, m))

    turnway = lax.rem(pos, 2)

    def space(kz, ky):
        return flip(z, kz) * ny + flip(y, ky)

    def along(kx, c):
        return flip(x, kx) * 2 + c

    sends = []

    def remote(a, b, s, r, to, when=None):
        cp = pltpu.make_async_remote_copy(a, b, s, r, device_id=to, device_id_type=MESH)
        cp.start()
        sends.append(cp)

    def arrived(ref, s, r):
        pltpu.make_async_remote_copy(
            ref, ref, s, r, device_id=(sp, pcore), device_id_type=MESH).wait_recv()

    def lanes(h):
        return pl.ds(pl.multiple_of(h * hh, LANES), hh)

    def deep(h):
        return pl.ds(pl.multiple_of(h * hh, LANES), hh)

    def block_rows(s):
        return pl.ds(pl.multiple_of(s * dblk, dblk), dblk)

    own = [
        pltpu.make_async_copy(qn_ref, qraw, local_sem.at[0]),
        pltpu.make_async_copy(ffin_ref.at[:, lanes(half)], fi.at[block_rows(sp)], local_sem.at[1]),
        pltpu.make_async_copy(ffout_ref.at[deep(half)], fo.at[sp], local_sem.at[2]),
        pltpu.make_async_copy(ow_ref, ow, local_sem.at[3]),
        pltpu.make_async_copy(kup_ref, kraw, local_sem.at[4]),
        pltpu.make_async_copy(vup_ref, vraw, local_sem.at[5]),
    ]
    for c in (1, 2, 0, 4, 5, 3):
        own[c].start()

    rope = rk_ref.shape[0]
    hw = rope // 2

    def turned(values):
        v = values.astype(F32)
        a, b = v[:hw], v[hw:]
        c, s = cos_ref[...], sin_ref[...]
        parts = [a * c - b * s, a * s + b * c]
        if rope % LANES:
            parts.append(jnp.zeros((-rope % LANES, rows), F32))
        return jnp.concatenate(parts, axis=0).T.astype(BF16)

    here = pl.ds(pl.multiple_of(sp * rows, rows), rows)
    full = lat_ref[...].astype(F32)
    spread_out = lax.rsqrt(jnp.mean(full * full, axis=-1, keepdims=True) + EPS)
    kv[here, pl.ds(0, latent_width)] = (full * spread_out * lgain_ref[...]).astype(BF16)
    kv[here, pl.ds(latent_width, kv.shape[1] - latent_width)] = turned(rk_ref[...])

    barrier = pltpu.get_barrier_semaphore()
    for i in range(1, n):
        pl.semaphore_signal(
            barrier, inc=1, device_id=(lax.rem(sp + i, n), me), device_id_type=MESH)
    for j in range(1, tp):
        pl.semaphore_signal(
            barrier, inc=1, device_id=(sp, lax.rem(me + j, tp)), device_id_type=MESH)
    pl.semaphore_wait(barrier, n + tp - 2)

    def piece(s, t):
        return kv.at[pl.ds(pl.multiple_of(s * rows + t * share, share), share)]

    def arrive(kz, ky):
        ref = piece(space(kz, ky), me)
        i = kz * ny + ky
        arrived(ref, ka_send.at[i], ka_recv.at[i])
        if ky == 0:
            for k in range(1, ny):
                j = kz * ny + k
                remote(ref, ref, ka_send.at[j], ka_recv.at[j], (space(0, k), me))
        for kx in range(1, nx):
            remote(ref, ref, kx_send.at[i, kx], kx_recv.at[i, kx], (sp, along(kx, core)))
        remote(ref, ref, kp_send.at[i, 0], kp_recv.at[i, 0], (sp, pcore))

    def across(kz, ky):
        i = kz * ny + ky
        for kx in range(1, nx):
            ref = piece(space(kz, ky), along(kx, core))
            arrived(ref, kx_send.at[i, kx], kx_recv.at[i, kx])
            remote(ref, ref, kp_send.at[i, kx], kp_recv.at[i, kx], (sp, pcore))

    def settle(kz, ky):
        i = kz * ny + ky
        for kx in range(nx):
            ref = piece(space(kz, ky), along(kx, 1 - core))
            arrived(ref, kp_send.at[i, kx], kp_recv.at[i, kx])

    def inner_of(h):
        return (hz - 1) * (1 - h)

    def is_inner(hm):
        return lax.div(lax.rem(hm, m), ny) == inner_of(half)

    def w_whole(b, s):
        return fi.at[block_rows(s)] if b == 0 else fo.at[s]

    def w_ref(b, s, way):
        if b == 0:
            return fi.at[pl.ds(pl.multiple_of(s * dblk + way * (dblk // 2), dblk // 2), dblk // 2)]
        return fo.at[s, pl.ds(pl.multiple_of(way * (hh // 2), hh // 2), hh // 2)]

    def home(way, step):
        return at((2 * way - 1) * step)

    def source(g, hm):
        if g == 0:
            return hm
        return (1 - half) * m + (g - 1) * ny + lax.rem(hm, ny)

    def cross(b):
        to = (1 - half) * m + inner_of(1 - half) * ny + y
        a = ffin_ref.at[:, lanes(1 - half)] if b == 0 else ffout_ref.at[deep(1 - half)]
        remote(a, w_whole(b, sp), c_send.at[b], c_recv.at[b, zl], (to, me))

    guarded = []

    def unit(b, g, step, k):
        way = turnway if k == 0 else 1 - turnway
        hm = home(way, step)
        s = source(g, hm)
        ref = w_ref(b, s, way)
        if step < m - 1:
            cp = pltpu.make_async_remote_copy(
                ref, ref, w_send.at[b, g, way, step], w_recv.at[b, g, way, step],
                device_id=(at(1 - 2 * way), me), device_id_type=MESH)

        def go():
            if step > 0:
                arrived(ref, w_send.at[b, g, way, step - 1], w_recv.at[b, g, way, step - 1])
            elif g > 0 and k == 0:
                arrived(w_whole(b, s), c_send.at[b], c_recv.at[b, g - 1])
            if step < m - 1:
                cp.start()

        if g == 0:
            go()
            if step < m - 1:
                sends.append(cp)
        else:
            pl.when(is_inner(hm))(go)
            if step < m - 1:
                guarded.append((hm, cp))

    others = range(1, hz + 1)
    issued = set()

    def do(b, g, step, k):
        if step < m and (b, g, step, k) not in issued:
            if step > 0:
                do(b, g, step - 1, k)
            issued.add((b, g, step, k))
            unit(b, g, step, k)

    def near(b, step, *ks):
        for k in ks:
            do(b, 0, step, k)

    def far(b, step, *ks):
        for k in ks:
            for g in others:
                do(b, g, step, k)

    mine = piece(sp, me)
    for ky in range(1, ny):
        remote(mine, mine, ka_send.at[ky], ka_recv.at[ky], (space(0, ky), me))
    for kz in range(1, nz):
        remote(mine, mine, ka_send.at[kz * ny], ka_recv.at[kz * ny], (space(kz, 0), me))
    own[1].wait()
    near(0, 0, 0, 1)

    scale = 1.0 / math.sqrt(LANES + rope)

    def score(kz):
        keys = pl.ds(pl.multiple_of(flip(z, kz) * chunk, chunk), chunk)

        def one(h, _):
            s = lax.dot_general(
                q[h], kv[keys, :], (((1,), (1,)), ((), ())),
                preferred_element_type=F32) * scale
            sc[kz, h] = s
            best = jnp.max(s, axis=1, keepdims=True)
            if kz > 0:
                best = jnp.maximum(best, top[h][:, :1])
            top[h] = jnp.broadcast_to(best, (rows, LANES))
            return 0

        lax.fori_loop(0, heads, one, 0)

    def unpack(raw, count):
        plain[pl.ds(0, count * heads), :] = raw[...].astype(F32)

    def head_rows(h, count):
        return plain[pl.ds(h, count, stride=heads), :].astype(BF16)

    own[0].wait()
    unpack(qraw, rows)
    for h in range(heads):
        q[h, :, pl.ds(0, vdim)] = head_rows(h, rows)
    own[4].wait()
    unpack(kraw, latent_width)
    for h in range(heads):
        q[h, :, pl.ds(0, latent_width)] = lax.dot_general(
            q[h, :, pl.ds(0, vdim)], head_rows(h, latent_width), (((1,), (1,)), ((), ())),
            preferred_element_type=F32).astype(BF16)
    for ky in range(1, ny):
        arrive(0, ky)
    arrive(1, 0)
    for h in range(heads):
        q[h, :, pl.ds(latent_width, q.shape[2] - latent_width)] = turned(qr_ref[h])
    own[5].wait()
    unpack(vraw, latent_width)
    for h in range(heads):
        vup[:, h * vdim:(h + 1) * vdim] = head_rows(h, latent_width)
    for ky in range(1, ny):
        across(0, ky)
    for kz in range(2, nz):
        arrive(kz, 0)
    own[2].wait()
    cross(0)
    near(1, 0, 0, 1)
    for ky in range(1, ny):
        settle(0, ky)
    for ky in range(1, ny):
        arrive(1, ky)
    score(0)
    for kz in range(1, nz):
        for ky in range(1, ny):
            if kz > 1:
                arrive(kz, ky)
    near(0, 1, 0)
    for kz in range(1, nz):
        for ky in range(ny):
            across(kz, ky)
        for ky in range(ny):
            settle(kz, ky)
        score(kz)
        if kz == 1:
            cross(1)
            near(1, 1, 0)
            near(0, 1, 1)
        elif kz == nz - 1:
            far(0, 0, 0, 1)

    squares = jnp.zeros((rows, 1), F32)
    for h in range(heads):
        peak = top[h][:, :1]
        acc[...] = jnp.zeros_like(acc)

        def gather(kz, den):
            zk = flip(z, 0)
            zk = jnp.where(kz == 0, z, zk)
            for k in range(1, nz):
                zk = jnp.where(kz == k, flip(z, k), zk)
            e = jnp.exp(sc[kz, h] - peak)
            acc[...] += jnp.dot(
                e.astype(BF16),
                kv[pl.ds(pl.multiple_of(zk * chunk, chunk), chunk), pl.ds(0, latent_width)],
                preferred_element_type=F32)
            return den + jnp.sum(e, axis=1, keepdims=True)

        den = lax.fori_loop(0, nz, gather, jnp.zeros((rows, 1), F32))
        lat = (acc[...] / den).astype(BF16)
        cols = slice(h * vdim, (h + 1) * vdim)
        one = jnp.dot(lat, vup[:, cols], preferred_element_type=F32)
        squares = squares + jnp.sum(one * one, axis=1, keepdims=True)
        scaled = (one * gain_ref[:, cols]).astype(BF16)
        for t in range(tp):
            gated[t % 2, (t // 2) * share:(t // 2 + 1) * share, cols] = (
                scaled[t * share:(t + 1) * share])
        if h == 0:
            near(0, 2, 0)
            near(1, 1, 1)
        elif h == heads // 2:
            near(0, 2, 1)
    sq_out[...] = jnp.broadcast_to(squares, sq_out.shape)
    own[3].wait()

    tile = width // 4

    def project(which, put):
        def one(c, _):
            cols = pl.ds(pl.multiple_of(c * tile, tile), tile)
            got = jnp.dot(gated[which], ow[:, cols], preferred_element_type=F32)
            put(cols, got.reshape(nx, share, tile))
            return 0
        lax.fori_loop(0, 4, one, 0)

    def put_out(cols, got):
        pout[:, :, cols] = got.astype(BF16)

    def put_keep(cols, got):
        keep[:, :, cols] = got

    project(1 - core, put_out)
    remote(pout, pin, r_send.at[0], r_recv.at[0], (sp, pcore))
    for j in range(1, tp):
        to = lax.rem(me + j, tp)
        remote(sq_out.at[pl.ds(pl.multiple_of(to * share, share), share)], sq_in.at[j],
               s_send.at[j], s_recv.at[j], (sp, to))
    project(core, put_keep)
    arrived(pin, r_send.at[0], r_recv.at[0])
    for kx in range(1, nx):
        xi = flip(x, kx)
        xout[kx - 1] = (keep[xi] + pin[xi].astype(F32)).astype(BF16)
        remote(xout.at[kx - 1], xin.at[kx - 1], r_send.at[kx], r_recv.at[kx], (sp, along(kx, core)))
    far(0, 1, 0, 1)
    far(1, 0, 0, 1)
    near(1, 2, 1)
    summed = keep[x] + pin[x].astype(F32)
    square = sq_out[pl.ds(pl.multiple_of(me * share, share), share)]
    for j in range(1, tp):
        arrived(sq_in.at[j], s_send.at[j], s_recv.at[j])
        square = square + sq_in[j]
    for kx in range(1, nx):
        arrived(xin.at[kx - 1], r_send.at[kx], r_recv.at[kx])
        summed = summed + xin[kx - 1].astype(F32)
    row_scale = lax.rsqrt(square[:, :1] / (heads * tp * vdim) + EPS)
    middle = stream_ref[...].astype(F32) + row_scale * summed
    mid[...] = middle
    norm = lax.rsqrt(jnp.mean(middle * middle, axis=1, keepdims=True) + EPS)

    def seat(kx, c):
        return c * nx + flip(x, kx)

    xs[0, seat(0, core)] = (middle * norm * ngain_ref[...]).astype(BF16)

    def hand(s, kx):
        ref = xs.at[s, seat(kx, core)]
        remote(ref, ref, g_send.at[1, s, kx], g_recv.at[1, s, kx], (sp, pcore))

    def spread(s):
        ref = xs.at[s, seat(0, core)]
        for kx in range(1, nx):
            remote(ref, ref, g_send.at[0, s, kx], g_recv.at[0, s, kx], (sp, along(kx, core)))
        hand(s, 0)

    def collect(s):
        for kx in range(1, nx):
            arrived(xs.at[s, seat(kx, core)], g_send.at[0, s, kx], g_recv.at[0, s, kx])
            hand(s, kx)

    def settled(s):
        for kx in range(nx):
            arrived(xs.at[s, seat(kx, 1 - core)], g_send.at[1, s, kx], g_recv.at[1, s, kx])

    ref = xs.at[0, seat(0, core)]
    remote(ref, xs.at[1, seat(0, core)], g_send.at[0, 0, 0], g_recv.at[0, 0, 0], (mate, me))
    spread(0)
    far(0, 2, 0, 1)
    near(0, m - 1, 0, 1)
    collect(0)
    settled(0)
    far(1, 1, 0)
    near(1, 2, 0)
    far(0, m - 1, 0, 1)

    wide = 512 if hh % 512 == 0 else 128

    def first(s):
        for c in range(hh // wide):
            cols = slice(c * wide, (c + 1) * wide)
            pre = jnp.dot(
                xs[s].reshape(rows, width), fi[:, cols], preferred_element_type=F32)
            pre = jnp.maximum(pre, 0.0)
            act[s, :, cols] = (pre * pre).astype(BF16)

    flow = []
    for k in range(m):
        flow.append((0, at(k)))
    for g in others:
        for ky in range(ny):
            flow.append((g, (1 - half) * m + (g - 1) * ny + flip(y, ky)))

    def stage_dot(i, u):
        got = jnp.dot(act[u], fo[flow[i][1]], preferred_element_type=F32)
        fresh[...] = got.reshape(2, nx, share, dblk)
        mixed[i, u] = fresh[core]
        mpo[i, u] = fresh[1 - core].astype(BF16)
        remote(mpo.at[i, u], mpi.at[i, u], mp_send.at[i, u], mp_recv.at[i, u], (sp, pcore))

    def stage_core(i, u):
        arrived(mpi.at[i, u], mp_send.at[i, u], mp_recv.at[i, u])
        for kx in range(1, nx):
            xi = flip(x, kx)
            mxo[i, u, kx - 1] = (
                mixed[i, u, xi] + mpi[i, u, xi].astype(F32)).astype(BF16)
            remote(mxo.at[i, u, kx - 1], mxi.at[i, u, kx - 1], mx_send.at[i, u, kx],
                   mx_recv.at[i, u, kx], (sp, along(kx, core)))

    def stage_x(i, u):
        s = flow[i][1]
        v = mixed[i, u, x] + mpi[i, u, x].astype(F32)
        for kx in range(1, nx):
            arrived(mxi.at[i, u, kx - 1], mx_send.at[i, u, kx], mx_recv.at[i, u, kx])
            v = v + mxi[i, u, kx - 1].astype(F32)
        if u == 1:
            mzo[s] = v.astype(BF16)
            remote(mzo.at[s], mzi.at[s], mz_send.at[s], mz_recv.at[s], (mate, me))
        else:
            cols = pl.ds(pl.multiple_of(s * dblk, dblk), dblk)
            mid[:, cols] = mid[:, cols] + v

    to_core, to_x = [], []

    def drain(cores, xs_left):
        while len(to_core) > cores:
            stage_core(*to_core[0])
            to_x.append(to_core.pop(0))
        while len(to_x) > xs_left:
            stage_x(*to_x.pop(0))

    def push(i, u):
        stage_dot(i, u)
        to_core.append((i, u))
        drain(2, 4)

    arrived(xs.at[1, seat(0, core)], g_send.at[0, 0, 0], g_recv.at[0, 0, 0])
    spread(1)
    far(1, 1, 1)
    first(0)
    early = [0, 2] if m == 4 else [0]
    late = [i for i in range(m) if i not in early]
    for i in early:
        push(i, 0)
    drain(0, 8)
    collect(1)
    far(1, 2, 0)
    far(1, 2, 1)
    settled(1)
    first(1)
    for i in early:
        push(i, 1)
    near(1, m - 1, 0, 1)
    for u in (1, 0):
        for i in late:
            push(i, u)
    for g in others:
        for k in range(2):
            do(1, g, m - 1, k)
        for u in (1, 0):
            for i in range(m, n):
                if flow[i][0] == g:
                    push(i, u)
    drain(0, 0)
    for i in range(n):
        s = flow[i][1]
        arrived(mzi.at[s], mz_send.at[s], mz_recv.at[s])
        cols = pl.ds(pl.multiple_of(s * dblk, dblk), dblk)
        out_ref[:, cols] = (mid[:, cols] + mzi[s].astype(F32)).astype(BF16)

    for cp in sends:
        cp.wait_send()
    for hm, cp in guarded:
        pl.when(is_inner(hm))(cp.wait_send)


def body(
    n, tp,
    stream, query_nope, query_rope, latent, rope_key, latent_gain,
    key_up, value_up, out_gain, out_weight, norm_gain, ff_in, ff_out,
):
    rows, heads = query_nope.shape[:2]
    width = stream.shape[1]
    latent_width = latent.shape[1]
    rope = rope_key.shape[1]
    dblk, hidden = ff_in.shape
    share = rows // tp
    positions = (lax.axis_index("sp") * rows + jnp.arange(rows, dtype=jnp.int32)).astype(F32)
    inverse = jnp.power(THETA, -jnp.arange(0, rope, 2, dtype=F32) / rope)
    angles = positions[None, :] * inverse[:, None]
    wide = latent_width + rope + (-rope) % LANES
    keys = n * rows
    nz, ny = ring_shape(n)
    hz, m, nx = nz // 2, n // 2, tp // 2
    chunk = ny * rows
    hh = hidden // 2
    vm = pl.BlockSpec(memory_space=pltpu.VMEM)
    hbm = pl.BlockSpec(memory_space=pl.ANY)
    dma = pltpu.SemaphoreType.DMA
    return pl.pallas_call(
        functools.partial(kernel, n, tp, heads, latent_width, width),
        out_shape=jax.ShapeDtypeStruct((share, width), BF16),
        in_specs=[vm, vm, vm, vm, vm, hbm, vm, hbm, hbm, vm, hbm, vm, vm, hbm, hbm],
        out_specs=vm,
        scratch_shapes=[
            pltpu.VMEM((rows * heads, LANES), BF16),
            pltpu.VMEM((latent_width * heads, LANES), BF16),
            pltpu.VMEM((latent_width * heads, LANES), BF16),
            pltpu.VMEM((max(rows, latent_width) * heads, LANES), F32),
            pltpu.VMEM((heads, rows, wide), BF16),
            pltpu.VMEM((latent_width, heads * LANES), BF16),
            pltpu.VMEM((keys, wide), BF16),
            pltpu.VMEM((width, hh), BF16),
            pltpu.VMEM((n, hh, dblk), BF16),
            pltpu.VMEM(out_weight.shape, BF16),
            pltpu.VMEM((nz, heads, rows, chunk), F32),
            pltpu.VMEM((heads, rows, LANES), F32),
            pltpu.VMEM((rows, latent_width), F32),
            pltpu.VMEM((2, nx * share, out_weight.shape[0]), BF16),
            pltpu.VMEM((nx, share, width), BF16),
            pltpu.VMEM((nx, share, width), BF16),
            pltpu.VMEM((nx, share, width), F32),
            pltpu.VMEM((max(nx - 1, 1), share, width), BF16),
            pltpu.VMEM((max(nx - 1, 1), share, width), BF16),
            pltpu.VMEM((rows, LANES), F32),
            pltpu.VMEM((tp, share, LANES), F32),
            pltpu.VMEM((share, width), F32),
            pltpu.VMEM((2, tp, share, width), BF16),
            pltpu.VMEM((2, rows, hh), BF16),
            pltpu.VMEM((2, nx, share, dblk), F32),
            pltpu.VMEM((n, 2, nx, share, dblk), F32),
            pltpu.VMEM((n, 2, nx, share, dblk), BF16),
            pltpu.VMEM((n, 2, nx, share, dblk), BF16),
            pltpu.VMEM((n, 2, max(nx - 1, 1), share, dblk), BF16),
            pltpu.VMEM((n, 2, max(nx - 1, 1), share, dblk), BF16),
            pltpu.VMEM((n, share, dblk), BF16),
            pltpu.VMEM((n, share, dblk), BF16),
            dma((6,)),
            dma((n,)), dma((n,)), dma((n, nx)), dma((n, nx)), dma((n, nx)), dma((n, nx)),
            dma((2,)), dma((2, hz)),
            dma((2, hz + 1, 2, m)), dma((2, hz + 1, 2, m)),
            dma((tp,)), dma((tp,)), dma((nx,)), dma((nx,)),
            dma((2, 2, nx)), dma((2, 2, nx)),
            dma((n, 2)), dma((n, 2)), dma((n, 2, nx)), dma((n, 2, nx)), dma((n,)), dma((n,)),
        ],
        compiler_params=pltpu.CompilerParams(
            collective_id=0, has_side_effects=True, vmem_limit_bytes=63 * 1024 * 1024
        ),
    )(
        latent, latent_gain[None, :], rope_key.T, jnp.cos(angles), jnp.sin(angles),
        query_nope.reshape(-1, LANES), query_rope.transpose(1, 2, 0),
        key_up.reshape(-1, LANES), value_up.reshape(-1, LANES), out_gain[None, :], out_weight,
        stream, norm_gain[None, :], ff_in, ff_out,
    )


def solution(mesh):
    placed = (
        P(("sp", "tp"), None),
        P("sp", "tp", None),
        P("sp", "tp", None),
        P("sp", None),
        P("sp", None),
        P(),
        P(None, "tp", None),
        P(None, "tp", None),
        P("tp"),
        P("tp", None),
        P(),
        P("sp", "tp"),
        P("tp", "sp"),
    )
    return jax.shard_map(
        functools.partial(body, mesh.shape["sp"], mesh.shape["tp"]),
        mesh=mesh, in_specs=placed, out_specs=P(("sp", "tp"), None), check_vma=False
    )
```

```python
import functools
import math

import jax
import jax.numpy as jnp
from jax import lax
from jax.experimental import pallas as pl
from jax.experimental.pallas import tpu as pltpu
from jax.sharding import PartitionSpec as P

EPS = 1e-06
THETA = 10000.0
F32 = jnp.float32
BF16 = jnp.bfloat16
MESH = pl.DeviceIdType.MESH
LANES = 128


def ring_shape(n):
    rows = 1
    while rows * rows < n:
        rows *= 2
    return (rows, n // rows) if n % rows == 0 else (n, 1)


def ring_pos(nz, ny, index):
    if ny == 1:
        return index
    z, y = lax.div(index, ny), lax.rem(index, ny)
    r = nz - 1 - z
    odd = lax.rem(r, 2)
    c = (1 - odd) * (y - 1) + odd * (ny - 1 - y)
    return jnp.where(y == 0, z, nz + r * (ny - 1) + c)


def ring_at(nz, ny, pos):
    if ny == 1:
        return pos
    q = jnp.maximum(pos - nz, 0)
    r, c = lax.div(q, ny - 1), lax.rem(q, ny - 1)
    odd = lax.rem(r, 2)
    y = 1 + (1 - odd) * c + odd * (ny - 2 - c)
    return jnp.where(pos < nz, pos * ny, (nz - 1 - r) * ny + y)


def flip(index, bits):
    bit = 1
    out = index
    while bit <= bits:
        if bits & bit:
            out = out + bit * (1 - 2 * lax.rem(lax.div(index, bit), 2))
        bit *= 2
    return out


def kernel(
    n, tp, heads, latent_width, width,
    lat_ref, lgain_ref, rk_ref, cos_ref, sin_ref, qn_ref, qr_ref, kup_ref, vup_ref,
    gain_ref, ow_ref, stream_ref, ngain_ref, ffin_ref, ffout_ref,
    out_ref,
    qraw, kraw, vraw, plain, rope_q, base, q, vup, kv, fi, fo, ow, sc, top, acc, gated, pout, pin, keep, xout, xin, sq_out, sq_in, mid, xs, act,
    fresh, mixed, mpo, mpi, mxo, mxi, mzo, mzi,
    local_sem, ka_send, ka_recv, kx_send, kx_recv, kp_send, kp_recv,
    c_send, c_recv, w_send, w_recv,
    s_send, s_recv, r_send, r_recv, g_send, g_recv,
    mp_send, mp_recv, mx_send, mx_recv, mz_send, mz_recv,
):
    sp = lax.axis_index("sp")
    me = lax.axis_index("tp")
    nz, ny = ring_shape(n)
    hz, m, nx = nz // 2, n // 2, tp // 2
    z, y = lax.div(sp, ny), lax.rem(sp, ny)
    x, core = lax.div(me, 2), lax.rem(me, 2)
    half, local = lax.div(sp, m), lax.rem(sp, m)
    zl = lax.div(local, ny)
    mate = lax.rem(sp + m, n)
    pcore = me + 1 - 2 * core
    rows = q.shape[1]
    share = rows // tp
    dblk = width // n
    hh = act.shape[2]
    chunk = sc.shape[2]
    vdim = LANES
    pos = ring_pos(hz, ny, local)

    def at(offset):
        return half * m + ring_at(hz, ny, lax.rem(pos + offset + m, m))

    turnway = lax.rem(pos, 2)

    def space(kz, ky):
        return flip(z, kz) * ny + flip(y, ky)

    def along(kx, c):
        return flip(x, kx) * 2 + c

    sends = []

    def remote(a, b, s, r, to, when=None):
        cp = pltpu.make_async_remote_copy(a, b, s, r, device_id=to, device_id_type=MESH)
        cp.start()
        sends.append(cp)

    def arrived(ref, s, r):
        pltpu.make_async_remote_copy(
            ref, ref, s, r, device_id=(sp, pcore), device_id_type=MESH).wait_recv()

    def lanes(h):
        return pl.ds(pl.multiple_of(h * hh, LANES), hh)

    def deep(h):
        return pl.ds(pl.multiple_of(h * hh, LANES), hh)

    def block_rows(s):
        return pl.ds(pl.multiple_of(s * dblk, dblk), dblk)

    barrier = pltpu.get_barrier_semaphore()
    for i in range(1, n):
        pl.semaphore_signal(
            barrier, inc=1, device_id=(lax.rem(sp + i, n), me), device_id_type=MESH)
    for j in range(1, tp):
        pl.semaphore_signal(
            barrier, inc=1, device_id=(sp, lax.rem(me + j, tp)), device_id_type=MESH)
    own = [
        pltpu.make_async_copy(qn_ref, qraw, local_sem.at[0]),
        pltpu.make_async_copy(ffin_ref.at[:, lanes(half)], fi.at[block_rows(sp)], local_sem.at[1]),
        pltpu.make_async_copy(ffout_ref.at[deep(half)], fo.at[sp], local_sem.at[2]),
        pltpu.make_async_copy(ow_ref, ow, local_sem.at[3]),
        pltpu.make_async_copy(kup_ref, kraw, local_sem.at[4]),
        pltpu.make_async_copy(vup_ref, vraw, local_sem.at[5]),
        pltpu.make_async_copy(qr_ref, rope_q, local_sem.at[6]),
        pltpu.make_async_copy(stream_ref, base, local_sem.at[7]),
    ]
    for c in (1, 2, 0, 4, 6, 5, 3, 7):
        own[c].start()

    rope = rk_ref.shape[0]
    hw = rope // 2

    def turned(values):
        v = values.astype(F32)
        a, b = v[:hw], v[hw:]
        c, s = cos_ref[...], sin_ref[...]
        parts = [a * c - b * s, a * s + b * c]
        if rope % LANES:
            parts.append(jnp.zeros((-rope % LANES, rows), F32))
        return jnp.concatenate(parts, axis=0).T.astype(BF16)

    here = pl.ds(pl.multiple_of(sp * rows, rows), rows)
    full = lat_ref[...].astype(F32)
    spread_out = lax.rsqrt(jnp.mean(full * full, axis=-1, keepdims=True) + EPS)
    kv[here, pl.ds(0, latent_width)] = (full * spread_out * lgain_ref[...]).astype(BF16)
    kv[here, pl.ds(latent_width, kv.shape[1] - latent_width)] = turned(rk_ref[...])

    pl.semaphore_wait(barrier, n + tp - 2)

    def piece(s, t):
        return kv.at[pl.ds(pl.multiple_of(s * rows + t * share, share), share)]

    def arrive(kz, ky):
        ref = piece(space(kz, ky), me)
        i = kz * ny + ky
        arrived(ref, ka_send.at[i], ka_recv.at[i])
        if ky == 0:
            for k in range(1, ny):
                j = kz * ny + k
                remote(ref, ref, ka_send.at[j], ka_recv.at[j], (space(0, k), me))
        for kx in range(1, nx):
            remote(ref, ref, kx_send.at[i, kx], kx_recv.at[i, kx], (sp, along(kx, core)))
        remote(ref, ref, kp_send.at[i, 0], kp_recv.at[i, 0], (sp, pcore))

    def across(kz, ky):
        i = kz * ny + ky
        for kx in range(1, nx):
            ref = piece(space(kz, ky), along(kx, core))
            arrived(ref, kx_send.at[i, kx], kx_recv.at[i, kx])
            remote(ref, ref, kp_send.at[i, kx], kp_recv.at[i, kx], (sp, pcore))

    def settle(kz, ky):
        i = kz * ny + ky
        for kx in range(nx):
            ref = piece(space(kz, ky), along(kx, 1 - core))
            arrived(ref, kp_send.at[i, kx], kp_recv.at[i, kx])

    def inner_of(h):
        return (hz - 1) * (1 - h)

    def is_inner(hm):
        return lax.div(lax.rem(hm, m), ny) == inner_of(half)

    def w_whole(b, s):
        return fi.at[block_rows(s)] if b == 0 else fo.at[s]

    def w_ref(b, s, way):
        if b == 0:
            return fi.at[pl.ds(pl.multiple_of(s * dblk + way * (dblk // 2), dblk // 2), dblk // 2)]
        return fo.at[s, pl.ds(pl.multiple_of(way * (hh // 2), hh // 2), hh // 2)]

    def home(way, step):
        return at((2 * way - 1) * step)

    def source(g, hm):
        if g == 0:
            return hm
        return (1 - half) * m + (g - 1) * ny + lax.rem(hm, ny)

    def cross(b):
        to = (1 - half) * m + inner_of(1 - half) * ny + y
        a = ffin_ref.at[:, lanes(1 - half)] if b == 0 else ffout_ref.at[deep(1 - half)]
        remote(a, w_whole(b, sp), c_send.at[b], c_recv.at[b, zl], (to, me))

    guarded = []

    def unit(b, g, step, k):
        way = turnway if k == 0 else 1 - turnway
        hm = home(way, step)
        s = source(g, hm)
        ref = w_ref(b, s, way)
        if step < m - 1:
            cp = pltpu.make_async_remote_copy(
                ref, ref, w_send.at[b, g, way, step], w_recv.at[b, g, way, step],
                device_id=(at(1 - 2 * way), me), device_id_type=MESH)

        def go():
            if step > 0:
                arrived(ref, w_send.at[b, g, way, step - 1], w_recv.at[b, g, way, step - 1])
            elif g > 0 and k == 0:
                arrived(w_whole(b, s), c_send.at[b], c_recv.at[b, g - 1])
            if step < m - 1:
                cp.start()

        if g == 0:
            go()
            if step < m - 1:
                sends.append(cp)
        else:
            pl.when(is_inner(hm))(go)
            if step < m - 1:
                guarded.append((hm, cp))

    others = range(1, hz + 1)
    issued = set()

    def do(b, g, step, k):
        if step < m and (b, g, step, k) not in issued:
            if step > 0:
                do(b, g, step - 1, k)
            issued.add((b, g, step, k))
            unit(b, g, step, k)

    def near(b, step, *ks):
        for k in ks:
            do(b, 0, step, k)

    def far(b, step, *ks, groups=None):
        for g in groups or others:
            for k in ks:
                do(b, g, step, k)

    mine = piece(sp, me)
    for ky in range(1, ny):
        remote(mine, mine, ka_send.at[ky], ka_recv.at[ky], (space(0, ky), me))
    for kz in range(1, nz):
        remote(mine, mine, ka_send.at[kz * ny], ka_recv.at[kz * ny], (space(kz, 0), me))
    own[1].wait()
    near(0, 0, 0, 1)

    scale = math.log2(math.e) / math.sqrt(LANES + rope)
    strip = 2 * LANES
    team = heads * rows

    def score(kz):
        base = flip(z, kz) * chunk

        def one(t, _):
            keys = pl.ds(pl.multiple_of(base + t * strip, strip), strip)
            s = lax.dot_general(
                q[...].reshape(team, q.shape[2]), kv[keys, :], (((1,), (1,)), ((), ())),
                preferred_element_type=F32) * scale
            sc[kz, :, pl.ds(pl.multiple_of(t * strip, strip), strip)] = s
            best = jnp.maximum(s[:, :LANES], s[:, LANES:])
            top[...] = jnp.maximum(top[...], best)
            return 0

        lax.fori_loop(0, chunk // strip, one, 0)

    top[...] = jnp.full(top.shape, -jnp.inf, F32)

    def unpack(raw, count):
        plain[pl.ds(0, count * heads), :] = raw[...].astype(F32)

    def head_rows(h, count):
        return plain[pl.ds(h, count, stride=heads), :].astype(BF16)

    own[0].wait()
    unpack(qraw, rows)
    for h in range(heads):
        q[h, :, pl.ds(0, vdim)] = head_rows(h, rows)
    own[4].wait()
    unpack(kraw, latent_width)
    for h in range(heads):
        q[h, :, pl.ds(0, latent_width)] = lax.dot_general(
            q[h, :, pl.ds(0, vdim)], head_rows(h, latent_width), (((1,), (1,)), ((), ())),
            preferred_element_type=F32).astype(BF16)
    for ky in range(1, ny):
        arrive(0, ky)
    arrive(1, 0)
    own[6].wait()
    for h in range(heads):
        q[h, :, pl.ds(latent_width, q.shape[2] - latent_width)] = turned(rope_q[h])
    own[5].wait()
    unpack(vraw, latent_width)
    for h in range(heads):
        vup[:, h * vdim:(h + 1) * vdim] = head_rows(h, latent_width)
    for ky in range(1, ny):
        across(0, ky)
    for kz in range(2, nz):
        arrive(kz, 0)
    own[2].wait()
    cross(0)
    near(1, 0, 0, 1)
    for ky in range(1, ny):
        settle(0, ky)
    for ky in range(1, ny):
        arrive(1, ky)
    score(0)
    for kz in range(1, nz):
        for ky in range(1, ny):
            if kz > 1:
                arrive(kz, ky)
    near(0, 1, 0)
    for kz in range(1, nz):
        for ky in range(ny):
            across(kz, ky)
        for ky in range(ny):
            settle(kz, ky)
        score(kz)
        if kz == 1:
            cross(1)
            near(1, 1, 0)
            near(0, 1, 1)
        elif kz == nz - 1:
            near(0, 2, 0)

    squares = jnp.zeros((rows, 1), F32)
    for h in range(heads):
        team_rows = slice(h * rows, (h + 1) * rows)
        peak = jnp.max(top[team_rows], axis=1, keepdims=True)
        acc[...] = jnp.zeros_like(acc)

        def gather(kz, den):
            zk = flip(z, 0)
            zk = jnp.where(kz == 0, z, zk)
            for k in range(1, nz):
                zk = jnp.where(kz == k, flip(z, k), zk)
            e = jnp.exp2(sc[kz, team_rows] - peak)
            acc[...] += jnp.dot(
                e.astype(BF16),
                kv[pl.ds(pl.multiple_of(zk * chunk, chunk), chunk), pl.ds(0, latent_width)],
                preferred_element_type=F32)
            return den + jnp.sum(e, axis=1, keepdims=True)

        den = lax.fori_loop(0, nz, gather, jnp.zeros((rows, 1), F32))
        lat = (acc[...] / den).astype(BF16)
        cols = slice(h * vdim, (h + 1) * vdim)
        one = jnp.dot(lat, vup[:, cols], preferred_element_type=F32)
        squares = squares + jnp.sum(one * one, axis=1, keepdims=True)
        scaled = (one * gain_ref[:, cols]).astype(BF16)
        for t in range(tp):
            gated[t % 2, (t // 2) * share:(t // 2 + 1) * share, cols] = (
                scaled[t * share:(t + 1) * share])
        if h == 0:
            near(1, 1, 1)
        if h == heads // 2 - 1:
            far(0, 0, 0, 1)
        if h == heads // 2:
            near(0, 2, 1)
    sq_out[...] = jnp.broadcast_to(squares, sq_out.shape)
    own[3].wait()

    tile = width // 4

    def project(which, put):
        def one(c, _):
            cols = pl.ds(pl.multiple_of(c * tile, tile), tile)
            got = jnp.dot(gated[which], ow[:, cols], preferred_element_type=F32)
            put(cols, got.reshape(nx, share, tile))
            return 0
        lax.fori_loop(0, 4, one, 0)

    def put_out(cols, got):
        pout[:, :, cols] = got.astype(BF16)

    def put_keep(cols, got):
        keep[:, :, cols] = got

    project(1 - core, put_out)
    remote(pout, pin, r_send.at[0], r_recv.at[0], (sp, pcore))
    for j in range(1, tp):
        to = lax.rem(me + j, tp)
        remote(sq_out.at[pl.ds(pl.multiple_of(to * share, share), share)], sq_in.at[j],
               s_send.at[j], s_recv.at[j], (sp, to))
    project(core, put_keep)
    arrived(pin, r_send.at[0], r_recv.at[0])
    for kx in range(1, nx):
        xi = flip(x, kx)
        xout[kx - 1] = (keep[xi] + pin[xi].astype(F32)).astype(BF16)
        remote(xout.at[kx - 1], xin.at[kx - 1], r_send.at[kx], r_recv.at[kx], (sp, along(kx, core)))
    far(0, 1, 0, 1)
    far(1, 0, 0, 1)
    near(1, 2, 1)
    summed = keep[x] + pin[x].astype(F32)
    square = sq_out[pl.ds(pl.multiple_of(me * share, share), share)]
    for j in range(1, tp):
        arrived(sq_in.at[j], s_send.at[j], s_recv.at[j])
        square = square + sq_in[j]
    for kx in range(1, nx):
        arrived(xin.at[kx - 1], r_send.at[kx], r_recv.at[kx])
        summed = summed + xin[kx - 1].astype(F32)
    row_scale = lax.rsqrt(square[:, :1] / (heads * tp * vdim) + EPS)
    own[7].wait()
    middle = base[...].astype(F32) + row_scale * summed
    mid[...] = middle
    norm = lax.rsqrt(jnp.mean(middle * middle, axis=1, keepdims=True) + EPS)

    def seat(kx, c):
        return c * nx + flip(x, kx)

    xs[0, seat(0, core)] = (middle * norm * ngain_ref[...]).astype(BF16)

    def hand(s, kx):
        ref = xs.at[s, seat(kx, core)]
        remote(ref, ref, g_send.at[1, s, kx], g_recv.at[1, s, kx], (sp, pcore))

    def spread(s):
        ref = xs.at[s, seat(0, core)]
        for kx in range(1, nx):
            remote(ref, ref, g_send.at[0, s, kx], g_recv.at[0, s, kx], (sp, along(kx, core)))
        hand(s, 0)

    def collect(s):
        for kx in range(1, nx):
            arrived(xs.at[s, seat(kx, core)], g_send.at[0, s, kx], g_recv.at[0, s, kx])
            hand(s, kx)

    def settled(s):
        for kx in range(nx):
            arrived(xs.at[s, seat(kx, 1 - core)], g_send.at[1, s, kx], g_recv.at[1, s, kx])

    ref = xs.at[0, seat(0, core)]
    remote(ref, xs.at[1, seat(0, core)], g_send.at[0, 0, 0], g_recv.at[0, 0, 0], (mate, me))
    spread(0)
    far(0, 2, 0, 1)
    near(0, m - 1, 0, 1)
    collect(0)
    settled(0)
    far(1, 1, 0)
    near(1, 2, 0)
    far(0, m - 1, 0, 1)

    wide = 512 if hh % 512 == 0 else 128

    def first(s):
        for c in range(hh // wide):
            cols = slice(c * wide, (c + 1) * wide)
            pre = jnp.dot(
                xs[s].reshape(rows, width), fi[:, cols], preferred_element_type=F32)
            pre = jnp.maximum(pre, 0.0)
            act[s, :, cols] = (pre * pre).astype(BF16)

    flow = []
    for k in range(m):
        flow.append((0, at(k)))
    for g in others:
        for ky in range(ny):
            flow.append((g, (1 - half) * m + (g - 1) * ny + flip(y, ky)))

    def stage_dot(i, u):
        got = jnp.dot(act[u], fo[flow[i][1]], preferred_element_type=F32)
        fresh[...] = got.reshape(2, nx, share, dblk)
        mixed[i, u] = fresh[core]
        mpo[i, u] = fresh[1 - core].astype(BF16)
        remote(mpo.at[i, u], mpi.at[i, u], mp_send.at[i, u], mp_recv.at[i, u], (sp, pcore))

    def stage_core(i, u):
        arrived(mpi.at[i, u], mp_send.at[i, u], mp_recv.at[i, u])
        for kx in range(1, nx):
            xi = flip(x, kx)
            mxo[i, u, kx - 1] = (
                mixed[i, u, xi] + mpi[i, u, xi].astype(F32)).astype(BF16)
            remote(mxo.at[i, u, kx - 1], mxi.at[i, u, kx - 1], mx_send.at[i, u, kx],
                   mx_recv.at[i, u, kx], (sp, along(kx, core)))

    def stage_x(i, u):
        s = flow[i][1]
        v = mixed[i, u, x] + mpi[i, u, x].astype(F32)
        for kx in range(1, nx):
            arrived(mxi.at[i, u, kx - 1], mx_send.at[i, u, kx], mx_recv.at[i, u, kx])
            v = v + mxi[i, u, kx - 1].astype(F32)
        if u == 1:
            mzo[s] = v.astype(BF16)
            remote(mzo.at[s], mzi.at[s], mz_send.at[s], mz_recv.at[s], (mate, me))
        else:
            cols = pl.ds(pl.multiple_of(s * dblk, dblk), dblk)
            mid[:, cols] = mid[:, cols] + v

    to_core, to_x = [], []

    def drain(cores, xs_left):
        while len(to_core) > cores:
            stage_core(*to_core[0])
            to_x.append(to_core.pop(0))
        while len(to_x) > xs_left:
            stage_x(*to_x.pop(0))

    def push(i, u):
        stage_dot(i, u)
        to_core.append((i, u))
        drain(2, 4)

    arrived(xs.at[1, seat(0, core)], g_send.at[0, 0, 0], g_recv.at[0, 0, 0])
    spread(1)
    far(1, 1, 1, groups=others[:1])
    first(0)
    far(1, 1, 1)
    early = [0, 2] if m == 4 else [0]
    late = [i for i in range(m) if i not in early]
    for i in early:
        push(i, 0)
    drain(0, 8)
    collect(1)
    far(1, 2, 0, 1, groups=others[:1])
    settled(1)
    first(1)
    for i in early:
        push(i, 1)
    far(1, 2, 0, 1)
    for g in others:
        if g == 2:
            near(1, m - 1, 0, 1)
            for u in (1, 0):
                for i in late:
                    push(i, u)
        for k in range(2):
            do(1, g, m - 1, k)
        for u in (1, 0):
            for i in range(m, n):
                if flow[i][0] == g:
                    push(i, u)
    drain(0, 0)
    for i in range(n):
        s = flow[i][1]
        arrived(mzi.at[s], mz_send.at[s], mz_recv.at[s])
        cols = pl.ds(pl.multiple_of(s * dblk, dblk), dblk)
        out_ref[:, cols] = (mid[:, cols] + mzi[s].astype(F32)).astype(BF16)

    for cp in sends:
        cp.wait_send()
    for hm, cp in guarded:
        pl.when(is_inner(hm))(cp.wait_send)


def body(
    n, tp,
    stream, query_nope, query_rope, latent, rope_key, latent_gain,
    key_up, value_up, out_gain, out_weight, norm_gain, ff_in, ff_out,
):
    rows, heads = query_nope.shape[:2]
    width = stream.shape[1]
    latent_width = latent.shape[1]
    rope = rope_key.shape[1]
    dblk, hidden = ff_in.shape
    share = rows // tp
    positions = (lax.axis_index("sp") * rows + jnp.arange(rows, dtype=jnp.int32)).astype(F32)
    inverse = jnp.power(THETA, -jnp.arange(0, rope, 2, dtype=F32) / rope)
    angles = positions[None, :] * inverse[:, None]
    wide = latent_width + rope + (-rope) % LANES
    keys = n * rows
    nz, ny = ring_shape(n)
    hz, m, nx = nz // 2, n // 2, tp // 2
    chunk = ny * rows
    hh = hidden // 2
    vm = pl.BlockSpec(memory_space=pltpu.VMEM)
    hbm = pl.BlockSpec(memory_space=pl.ANY)
    dma = pltpu.SemaphoreType.DMA
    return pl.pallas_call(
        functools.partial(kernel, n, tp, heads, latent_width, width),
        out_shape=jax.ShapeDtypeStruct((share, width), BF16),
        in_specs=[vm, vm, vm, vm, vm, hbm, hbm, hbm, hbm, vm, hbm, hbm, vm, hbm, hbm],
        out_specs=vm,
        scratch_shapes=[
            pltpu.VMEM((rows * heads, LANES), BF16),
            pltpu.VMEM((latent_width * heads, LANES), BF16),
            pltpu.VMEM((latent_width * heads, LANES), BF16),
            pltpu.VMEM((max(rows, latent_width) * heads, LANES), F32),
            pltpu.VMEM((heads, rope, rows), BF16),
            pltpu.VMEM((share, width), BF16),
            pltpu.VMEM((heads, rows, wide), BF16),
            pltpu.VMEM((latent_width, heads * LANES), BF16),
            pltpu.VMEM((keys, wide), BF16),
            pltpu.VMEM((width, hh), BF16),
            pltpu.VMEM((n, hh, dblk), BF16),
            pltpu.VMEM(out_weight.shape, BF16),
            pltpu.VMEM((nz, heads * rows, chunk), F32),
            pltpu.VMEM((heads * rows, LANES), F32),
            pltpu.VMEM((rows, latent_width), F32),
            pltpu.VMEM((2, nx * share, out_weight.shape[0]), BF16),
            pltpu.VMEM((nx, share, width), BF16),
            pltpu.VMEM((nx, share, width), BF16),
            pltpu.VMEM((nx, share, width), F32),
            pltpu.VMEM((max(nx - 1, 1), share, width), BF16),
            pltpu.VMEM((max(nx - 1, 1), share, width), BF16),
            pltpu.VMEM((rows, LANES), F32),
            pltpu.VMEM((tp, share, LANES), F32),
            pltpu.VMEM((share, width), F32),
            pltpu.VMEM((2, tp, share, width), BF16),
            pltpu.VMEM((2, rows, hh), BF16),
            pltpu.VMEM((2, nx, share, dblk), F32),
            pltpu.VMEM((n, 2, nx, share, dblk), F32),
            pltpu.VMEM((n, 2, nx, share, dblk), BF16),
            pltpu.VMEM((n, 2, nx, share, dblk), BF16),
            pltpu.VMEM((n, 2, max(nx - 1, 1), share, dblk), BF16),
            pltpu.VMEM((n, 2, max(nx - 1, 1), share, dblk), BF16),
            pltpu.VMEM((n, share, dblk), BF16),
            pltpu.VMEM((n, share, dblk), BF16),
            dma((8,)),
            dma((n,)), dma((n,)), dma((n, nx)), dma((n, nx)), dma((n, nx)), dma((n, nx)),
            dma((2,)), dma((2, hz)),
            dma((2, hz + 1, 2, m)), dma((2, hz + 1, 2, m)),
            dma((tp,)), dma((tp,)), dma((nx,)), dma((nx,)),
            dma((2, 2, nx)), dma((2, 2, nx)),
            dma((n, 2)), dma((n, 2)), dma((n, 2, nx)), dma((n, 2, nx)), dma((n,)), dma((n,)),
        ],
        compiler_params=pltpu.CompilerParams(
            collective_id=0, has_side_effects=True, vmem_limit_bytes=63 * 1024 * 1024
        ),
    )(
        latent, latent_gain[None, :], rope_key.T, jnp.cos(angles), jnp.sin(angles),
        query_nope.reshape(-1, LANES), query_rope.transpose(1, 2, 0),
        key_up.reshape(-1, LANES), value_up.reshape(-1, LANES), out_gain[None, :], out_weight,
        stream, norm_gain[None, :], ff_in, ff_out,
    )


def solution(mesh):
    placed = (
        P(("sp", "tp"), None),
        P("sp", "tp", None),
        P("sp", "tp", None),
        P("sp", None),
        P("sp", None),
        P(),
        P(None, "tp", None),
        P(None, "tp", None),
        P("tp"),
        P("tp", None),
        P(),
        P("sp", "tp"),
        P("tp", "sp"),
    )
    return jax.shard_map(
        functools.partial(body, mesh.shape["sp"], mesh.shape["tp"]),
        mesh=mesh, in_specs=placed, out_specs=P(("sp", "tp"), None), check_vma=False
    )
```

```python
import functools
import math

import jax
import jax.numpy as jnp
from jax import lax
from jax.experimental import pallas as pl
from jax.experimental.pallas import tpu as pltpu
from jax.sharding import PartitionSpec as P

EPS = 1e-06
THETA = 10000.0
F32 = jnp.float32
BF16 = jnp.bfloat16
MESH = pl.DeviceIdType.MESH
LANES = 128


def ring_shape(n):
    rows = 1
    while rows * rows < n:
        rows *= 2
    return (rows, n // rows) if n % rows == 0 else (n, 1)


def ring_pos(nz, ny, index):
    if ny == 1:
        return index
    z, y = lax.div(index, ny), lax.rem(index, ny)
    r = nz - 1 - z
    odd = lax.rem(r, 2)
    c = (1 - odd) * (y - 1) + odd * (ny - 1 - y)
    return jnp.where(y == 0, z, nz + r * (ny - 1) + c)


def ring_at(nz, ny, pos):
    if ny == 1:
        return pos
    q = jnp.maximum(pos - nz, 0)
    r, c = lax.div(q, ny - 1), lax.rem(q, ny - 1)
    odd = lax.rem(r, 2)
    y = 1 + (1 - odd) * c + odd * (ny - 2 - c)
    return jnp.where(pos < nz, pos * ny, (nz - 1 - r) * ny + y)


def flip(index, bits):
    bit = 1
    out = index
    while bit <= bits:
        if bits & bit:
            out = out + bit * (1 - 2 * lax.rem(lax.div(index, bit), 2))
        bit *= 2
    return out


def kernel(
    n, tp, heads, latent_width, width,
    lat_ref, lgain_ref, rk_ref, cos_ref, sin_ref, qn_ref, qr_ref, kup_ref, vup_ref,
    gain_ref, ow_ref, stream_ref, ngain_ref, ffin_ref, ffout_ref,
    out_ref,
    qraw, kraw, vraw, plain, rope_q, base, q, vup, kv, fi, fo, ow, sc, top, acc, gated, pout, pin, keep, xout, xin, sq_out, sq_in, mid, xs, act,
    fresh, mixed, mpo, mpi, mxo, mxi, mzo, mzi,
    local_sem, ka_send, ka_recv, kx_send, kx_recv, kp_send, kp_recv,
    c_send, c_recv, w_send, w_recv,
    s_send, s_recv, r_send, r_recv, g_send, g_recv,
    mp_send, mp_recv, mx_send, mx_recv, mz_send, mz_recv,
):
    sp = lax.axis_index("sp")
    me = lax.axis_index("tp")
    nz, ny = ring_shape(n)
    hz, m, nx = nz // 2, n // 2, tp // 2
    z, y = lax.div(sp, ny), lax.rem(sp, ny)
    x, core = lax.div(me, 2), lax.rem(me, 2)
    half, local = lax.div(sp, m), lax.rem(sp, m)
    zl = lax.div(local, ny)
    mate = lax.rem(sp + m, n)
    pcore = me + 1 - 2 * core
    rows = q.shape[1]
    share = rows // tp
    dblk = width // n
    hh = act.shape[2]
    chunk = sc.shape[2]
    vdim = LANES
    pos = ring_pos(hz, ny, local)

    def at(offset):
        return half * m + ring_at(hz, ny, lax.rem(pos + offset + m, m))

    turnway = lax.rem(pos, 2)

    def space(kz, ky):
        return flip(z, kz) * ny + flip(y, ky)

    def along(kx, c):
        return flip(x, kx) * 2 + c

    sends = []

    def remote(a, b, s, r, to, when=None):
        cp = pltpu.make_async_remote_copy(a, b, s, r, device_id=to, device_id_type=MESH)
        cp.start()
        sends.append(cp)

    def arrived(ref, s, r):
        pltpu.make_async_remote_copy(
            ref, ref, s, r, device_id=(sp, pcore), device_id_type=MESH).wait_recv()

    def lanes(h):
        return pl.ds(pl.multiple_of(h * hh, LANES), hh)

    def deep(h):
        return pl.ds(pl.multiple_of(h * hh, LANES), hh)

    def block_rows(s):
        return pl.ds(pl.multiple_of(s * dblk, dblk), dblk)

    barrier = pltpu.get_barrier_semaphore()
    for i in range(1, n):
        pl.semaphore_signal(
            barrier, inc=1, device_id=(lax.rem(sp + i, n), me), device_id_type=MESH)
    for j in range(1, tp):
        pl.semaphore_signal(
            barrier, inc=1, device_id=(sp, lax.rem(me + j, tp)), device_id_type=MESH)
    own = [
        pltpu.make_async_copy(qn_ref, qraw, local_sem.at[0]),
        pltpu.make_async_copy(ffin_ref.at[:, lanes(half)], fi.at[block_rows(sp)], local_sem.at[1]),
        pltpu.make_async_copy(ffout_ref.at[deep(half)], fo.at[sp], local_sem.at[2]),
        pltpu.make_async_copy(ow_ref, ow, local_sem.at[3]),
        pltpu.make_async_copy(kup_ref, kraw, local_sem.at[4]),
        pltpu.make_async_copy(vup_ref, vraw, local_sem.at[5]),
        pltpu.make_async_copy(qr_ref, rope_q, local_sem.at[6]),
        pltpu.make_async_copy(stream_ref, base, local_sem.at[7]),
    ]
    for c in (1, 2, 0, 4, 6, 5, 3, 7):
        own[c].start()

    rope = rk_ref.shape[0]
    hw = rope // 2

    def turned(values):
        v = values.astype(F32)
        a, b = v[:hw], v[hw:]
        c, s = cos_ref[...], sin_ref[...]
        parts = [a * c - b * s, a * s + b * c]
        if rope % LANES:
            parts.append(jnp.zeros((-rope % LANES, rows), F32))
        return jnp.concatenate(parts, axis=0).T.astype(BF16)

    here = pl.ds(pl.multiple_of(sp * rows, rows), rows)
    full = lat_ref[...].astype(F32)
    spread_out = lax.rsqrt(jnp.mean(full * full, axis=-1, keepdims=True) + EPS)
    kv[here, pl.ds(0, latent_width)] = (full * spread_out * lgain_ref[...]).astype(BF16)
    kv[here, pl.ds(latent_width, kv.shape[1] - latent_width)] = turned(rk_ref[...])

    pl.semaphore_wait(barrier, n + tp - 2)

    def piece(s, t):
        return kv.at[pl.ds(pl.multiple_of(s * rows + t * share, share), share)]

    def arrive(kz, ky):
        ref = piece(space(kz, ky), me)
        i = kz * ny + ky
        arrived(ref, ka_send.at[i], ka_recv.at[i])
        if ky == 0:
            for k in range(1, ny):
                j = kz * ny + k
                remote(ref, ref, ka_send.at[j], ka_recv.at[j], (space(0, k), me))
        for kx in range(1, nx):
            remote(ref, ref, kx_send.at[i, kx], kx_recv.at[i, kx], (sp, along(kx, core)))
        remote(ref, ref, kp_send.at[i, 0], kp_recv.at[i, 0], (sp, pcore))

    def across(kz, ky):
        i = kz * ny + ky
        for kx in range(1, nx):
            ref = piece(space(kz, ky), along(kx, core))
            arrived(ref, kx_send.at[i, kx], kx_recv.at[i, kx])
            remote(ref, ref, kp_send.at[i, kx], kp_recv.at[i, kx], (sp, pcore))

    def settle(kz, ky):
        i = kz * ny + ky
        for kx in range(nx):
            ref = piece(space(kz, ky), along(kx, 1 - core))
            arrived(ref, kp_send.at[i, kx], kp_recv.at[i, kx])

    def inner_of(h):
        return (hz - 1) * (1 - h)

    def is_inner(hm):
        return lax.div(lax.rem(hm, m), ny) == inner_of(half)

    def w_whole(b, s):
        return fi.at[block_rows(s)] if b == 0 else fo.at[s]

    def w_ref(b, s, way):
        if b == 0:
            return fi.at[pl.ds(pl.multiple_of(s * dblk + way * (dblk // 2), dblk // 2), dblk // 2)]
        return fo.at[s, pl.ds(pl.multiple_of(way * (hh // 2), hh // 2), hh // 2)]

    def home(way, step):
        return at((2 * way - 1) * step)

    def source(g, hm):
        if g == 0:
            return hm
        return (1 - half) * m + (g - 1) * ny + lax.rem(hm, ny)

    def cross(b):
        to = (1 - half) * m + inner_of(1 - half) * ny + y
        a = ffin_ref.at[:, lanes(1 - half)] if b == 0 else ffout_ref.at[deep(1 - half)]
        remote(a, w_whole(b, sp), c_send.at[b], c_recv.at[b, zl], (to, me))

    guarded = []

    def unit(b, g, step, k):
        way = turnway if k == 0 else 1 - turnway
        hm = home(way, step)
        s = source(g, hm)
        ref = w_ref(b, s, way)
        if step < m - 1:
            cp = pltpu.make_async_remote_copy(
                ref, ref, w_send.at[b, g, way, step], w_recv.at[b, g, way, step],
                device_id=(at(1 - 2 * way), me), device_id_type=MESH)

        def go():
            if step > 0:
                arrived(ref, w_send.at[b, g, way, step - 1], w_recv.at[b, g, way, step - 1])
            elif g > 0 and k == 0:
                arrived(w_whole(b, s), c_send.at[b], c_recv.at[b, g - 1])
            if step < m - 1:
                cp.start()

        if g == 0:
            go()
            if step < m - 1:
                sends.append(cp)
        else:
            pl.when(is_inner(hm))(go)
            if step < m - 1:
                guarded.append((hm, cp))

    others = range(1, hz + 1)
    issued = set()

    def do(b, g, step, k):
        if step < m and (b, g, step, k) not in issued:
            if step > 0:
                do(b, g, step - 1, k)
            issued.add((b, g, step, k))
            unit(b, g, step, k)

    def near(b, step, *ks):
        for k in ks:
            do(b, 0, step, k)

    def far(b, step, *ks, groups=None):
        for g in groups or others:
            for k in ks:
                do(b, g, step, k)

    mine = piece(sp, me)
    for ky in range(1, ny):
        remote(mine, mine, ka_send.at[ky], ka_recv.at[ky], (space(0, ky), me))
    for kz in range(1, nz):
        remote(mine, mine, ka_send.at[kz * ny], ka_recv.at[kz * ny], (space(kz, 0), me))
    own[1].wait()
    near(0, 0, 0, 1)

    scale = math.log2(math.e) / math.sqrt(LANES + rope)
    strip = 2 * LANES
    team = heads * rows

    def score(kz):
        base = flip(z, kz) * chunk

        def one(t, _):
            keys = pl.ds(pl.multiple_of(base + t * strip, strip), strip)
            s = lax.dot_general(
                q[...].reshape(team, q.shape[2]), kv[keys, :], (((1,), (1,)), ((), ())),
                preferred_element_type=F32) * scale
            sc[kz, :, pl.ds(pl.multiple_of(t * strip, strip), strip)] = s
            best = jnp.maximum(s[:, :LANES], s[:, LANES:])
            top[...] = jnp.maximum(top[...], best)
            return 0

        lax.fori_loop(0, chunk // strip, one, 0)

    top[...] = jnp.full(top.shape, -jnp.inf, F32)

    def unpack(raw, count):
        plain[pl.ds(0, count * heads), :] = raw[...].astype(F32)

    def head_rows(h, count):
        return plain[pl.ds(h, count, stride=heads), :].astype(BF16)

    own[0].wait()
    unpack(qraw, rows)
    for h in range(heads):
        q[h, :, pl.ds(0, vdim)] = head_rows(h, rows)
    own[4].wait()
    unpack(kraw, latent_width)
    for h in range(heads):
        q[h, :, pl.ds(0, latent_width)] = lax.dot_general(
            q[h, :, pl.ds(0, vdim)], head_rows(h, latent_width), (((1,), (1,)), ((), ())),
            preferred_element_type=F32).astype(BF16)
    for ky in range(1, ny):
        arrive(0, ky)
    arrive(1, 0)
    own[6].wait()
    for h in range(heads):
        q[h, :, pl.ds(latent_width, q.shape[2] - latent_width)] = turned(rope_q[h])
    own[5].wait()
    unpack(vraw, latent_width)
    for h in range(heads):
        vup[:, h * vdim:(h + 1) * vdim] = head_rows(h, latent_width)
    for ky in range(1, ny):
        across(0, ky)
    for kz in range(2, nz):
        arrive(kz, 0)
    own[2].wait()
    cross(0)
    near(1, 0, 0, 1)
    for ky in range(1, ny):
        settle(0, ky)
    for ky in range(1, ny):
        arrive(1, ky)
    score(0)
    for kz in range(1, nz):
        for ky in range(1, ny):
            if kz > 1:
                arrive(kz, ky)
    near(0, 1, 0)
    for kz in range(1, nz):
        for ky in range(ny):
            across(kz, ky)
        for ky in range(ny):
            settle(kz, ky)
        score(kz)
        if kz == 1:
            cross(1)
            near(1, 1, 0)
            near(0, 1, 1)
        elif kz == nz - 1:
            near(0, 2, 0)

    squares = jnp.zeros((rows, 1), F32)
    for h in range(heads):
        team_rows = slice(h * rows, (h + 1) * rows)
        peak = jnp.max(top[team_rows], axis=1, keepdims=True)
        acc[...] = jnp.zeros_like(acc)

        def gather(kz, den):
            zk = flip(z, 0)
            zk = jnp.where(kz == 0, z, zk)
            for k in range(1, nz):
                zk = jnp.where(kz == k, flip(z, k), zk)
            e = jnp.exp2(sc[kz, team_rows] - peak)
            acc[...] += jnp.dot(
                e.astype(BF16),
                kv[pl.ds(pl.multiple_of(zk * chunk, chunk), chunk), pl.ds(0, latent_width)],
                preferred_element_type=F32)
            return den + jnp.sum(e, axis=1, keepdims=True)

        den = lax.fori_loop(0, nz, gather, jnp.zeros((rows, 1), F32))
        lat = (acc[...] / den).astype(BF16)
        cols = slice(h * vdim, (h + 1) * vdim)
        one = jnp.dot(lat, vup[:, cols], preferred_element_type=F32)
        squares = squares + jnp.sum(one * one, axis=1, keepdims=True)
        scaled = (one * gain_ref[:, cols]).astype(BF16)
        for t in range(tp):
            gated[t % 2, (t // 2) * share:(t // 2 + 1) * share, cols] = (
                scaled[t * share:(t + 1) * share])
        if h == 0:
            near(1, 1, 1)
        if h == heads // 2 - 1:
            far(0, 0, 0, 1)
        if h == heads // 2:
            near(0, 2, 1)
    sq_out[...] = jnp.broadcast_to(squares, sq_out.shape)
    own[3].wait()

    tile = width // 4

    def project(which, put):
        def one(c, _):
            cols = pl.ds(pl.multiple_of(c * tile, tile), tile)
            got = jnp.dot(gated[which], ow[:, cols], preferred_element_type=F32)
            put(cols, got.reshape(nx, share, tile))
            return 0
        lax.fori_loop(0, 4, one, 0)

    def put_out(cols, got):
        pout[:, :, cols] = got.astype(BF16)

    def put_keep(cols, got):
        keep[:, :, cols] = got

    project(1 - core, put_out)
    remote(pout, pin, r_send.at[0], r_recv.at[0], (sp, pcore))
    for j in range(1, tp):
        to = lax.rem(me + j, tp)
        remote(sq_out.at[pl.ds(pl.multiple_of(to * share, share), share)], sq_in.at[j],
               s_send.at[j], s_recv.at[j], (sp, to))
    project(core, put_keep)
    arrived(pin, r_send.at[0], r_recv.at[0])
    for kx in range(1, nx):
        xi = flip(x, kx)
        xout[kx - 1] = (keep[xi] + pin[xi].astype(F32)).astype(BF16)
        remote(xout.at[kx - 1], xin.at[kx - 1], r_send.at[kx], r_recv.at[kx], (sp, along(kx, core)))
    far(0, 1, 0, 1)
    near(1, 2, 1)
    summed = keep[x] + pin[x].astype(F32)
    square = sq_out[pl.ds(pl.multiple_of(me * share, share), share)]
    for j in range(1, tp):
        arrived(sq_in.at[j], s_send.at[j], s_recv.at[j])
        square = square + sq_in[j]
    for kx in range(1, nx):
        arrived(xin.at[kx - 1], r_send.at[kx], r_recv.at[kx])
        summed = summed + xin[kx - 1].astype(F32)
    row_scale = lax.rsqrt(square[:, :1] / (heads * tp * vdim) + EPS)
    own[7].wait()
    middle = base[...].astype(F32) + row_scale * summed
    mid[...] = middle
    norm = lax.rsqrt(jnp.mean(middle * middle, axis=1, keepdims=True) + EPS)

    def seat(kx, c):
        return c * nx + flip(x, kx)

    xs[0, seat(0, core)] = (middle * norm * ngain_ref[...]).astype(BF16)

    def hand(s, kx):
        ref = xs.at[s, seat(kx, core)]
        remote(ref, ref, g_send.at[1, s, kx], g_recv.at[1, s, kx], (sp, pcore))

    def spread(s):
        ref = xs.at[s, seat(0, core)]
        for kx in range(1, nx):
            remote(ref, ref, g_send.at[0, s, kx], g_recv.at[0, s, kx], (sp, along(kx, core)))
        hand(s, 0)

    def collect(s):
        for kx in range(1, nx):
            arrived(xs.at[s, seat(kx, core)], g_send.at[0, s, kx], g_recv.at[0, s, kx])
            hand(s, kx)

    def settled(s):
        for kx in range(nx):
            arrived(xs.at[s, seat(kx, 1 - core)], g_send.at[1, s, kx], g_recv.at[1, s, kx])

    ref = xs.at[0, seat(0, core)]
    remote(ref, xs.at[1, seat(0, core)], g_send.at[0, 0, 0], g_recv.at[0, 0, 0], (mate, me))
    spread(0)
    far(1, 0, 0, 1)
    far(0, 2, 0, 1)
    near(0, m - 1, 0, 1)
    collect(0)
    settled(0)
    far(1, 1, 0)
    near(1, 2, 0)
    far(0, m - 1, 0, 1)

    wide = 512 if hh % 512 == 0 else 128

    def first(s):
        for c in range(hh // wide):
            cols = slice(c * wide, (c + 1) * wide)
            pre = jnp.dot(
                xs[s].reshape(rows, width), fi[:, cols], preferred_element_type=F32)
            pre = jnp.maximum(pre, 0.0)
            act[s, :, cols] = (pre * pre).astype(BF16)

    flow = []
    for k in range(m):
        flow.append((0, at(k)))
    for g in others:
        for ky in range(ny):
            flow.append((g, (1 - half) * m + (g - 1) * ny + flip(y, ky)))

    def stage_dot(i, u):
        got = jnp.dot(act[u], fo[flow[i][1]], preferred_element_type=F32)
        fresh[...] = got.reshape(2, nx, share, dblk)
        mixed[i, u] = fresh[core]
        mpo[i, u] = fresh[1 - core].astype(BF16)
        remote(mpo.at[i, u], mpi.at[i, u], mp_send.at[i, u], mp_recv.at[i, u], (sp, pcore))

    def stage_core(i, u):
        arrived(mpi.at[i, u], mp_send.at[i, u], mp_recv.at[i, u])
        for kx in range(1, nx):
            xi = flip(x, kx)
            mxo[i, u, kx - 1] = (
                mixed[i, u, xi] + mpi[i, u, xi].astype(F32)).astype(BF16)
            remote(mxo.at[i, u, kx - 1], mxi.at[i, u, kx - 1], mx_send.at[i, u, kx],
                   mx_recv.at[i, u, kx], (sp, along(kx, core)))

    def stage_x(i, u):
        s = flow[i][1]
        v = mixed[i, u, x] + mpi[i, u, x].astype(F32)
        for kx in range(1, nx):
            arrived(mxi.at[i, u, kx - 1], mx_send.at[i, u, kx], mx_recv.at[i, u, kx])
            v = v + mxi[i, u, kx - 1].astype(F32)
        if u == 1:
            mzo[s] = v.astype(BF16)
            remote(mzo.at[s], mzi.at[s], mz_send.at[s], mz_recv.at[s], (mate, me))
        else:
            cols = pl.ds(pl.multiple_of(s * dblk, dblk), dblk)
            mid[:, cols] = mid[:, cols] + v

    to_core, to_x = [], []

    def drain(cores, xs_left):
        while len(to_core) > cores:
            stage_core(*to_core[0])
            to_x.append(to_core.pop(0))
        while len(to_x) > xs_left:
            stage_x(*to_x.pop(0))

    def push(i, u):
        stage_dot(i, u)
        to_core.append((i, u))
        drain(1, 3)

    arrived(xs.at[1, seat(0, core)], g_send.at[0, 0, 0], g_recv.at[0, 0, 0])
    spread(1)
    far(1, 1, 1, groups=others[:1])
    first(0)
    far(1, 1, 1)
    early = [0, 2] if m == 4 else [0]
    late = [i for i in range(m) if i not in early]
    for i in early:
        push(i, 0)
    drain(0, 8)
    collect(1)
    far(1, 2, 0, 1, groups=others[:1])
    settled(1)
    first(1)
    for i in early:
        push(i, 1)
    far(1, 2, 0, 1)
    rest = list(late)
    for g in others:
        mine_g = [i for i in range(m, n) if flow[i][0] == g]
        for k in range(2):
            do(1, g, m - 1, k)
        for i in mine_g:
            push(i, 1)
        if g == 1:
            near(1, m - 1, 0, 1)
            for i in late:
                push(i, 1)
            for i in mine_g[:ny]:
                push(i, 0)
            rest += mine_g[ny:]
        else:
            rest += mine_g
    for i in rest:
        push(i, 0)
    drain(0, 0)
    for i in range(n):
        s = flow[i][1]
        arrived(mzi.at[s], mz_send.at[s], mz_recv.at[s])
        cols = pl.ds(pl.multiple_of(s * dblk, dblk), dblk)
        out_ref[:, cols] = (mid[:, cols] + mzi[s].astype(F32)).astype(BF16)

    for cp in sends:
        cp.wait_send()
    for hm, cp in guarded:
        pl.when(is_inner(hm))(cp.wait_send)


def body(
    n, tp,
    stream, query_nope, query_rope, latent, rope_key, latent_gain,
    key_up, value_up, out_gain, out_weight, norm_gain, ff_in, ff_out,
):
    rows, heads = query_nope.shape[:2]
    width = stream.shape[1]
    latent_width = latent.shape[1]
    rope = rope_key.shape[1]
    dblk, hidden = ff_in.shape
    share = rows // tp
    positions = (lax.axis_index("sp") * rows + jnp.arange(rows, dtype=jnp.int32)).astype(F32)
    inverse = jnp.power(THETA, -jnp.arange(0, rope, 2, dtype=F32) / rope)
    angles = positions[None, :] * inverse[:, None]
    wide = latent_width + rope + (-rope) % LANES
    keys = n * rows
    nz, ny = ring_shape(n)
    hz, m, nx = nz // 2, n // 2, tp // 2
    chunk = ny * rows
    hh = hidden // 2
    vm = pl.BlockSpec(memory_space=pltpu.VMEM)
    hbm = pl.BlockSpec(memory_space=pl.ANY)
    dma = pltpu.SemaphoreType.DMA
    return pl.pallas_call(
        functools.partial(kernel, n, tp, heads, latent_width, width),
        out_shape=jax.ShapeDtypeStruct((share, width), BF16),
        in_specs=[vm, vm, vm, vm, vm, hbm, hbm, hbm, hbm, vm, hbm, hbm, vm, hbm, hbm],
        out_specs=vm,
        scratch_shapes=[
            pltpu.VMEM((rows * heads, LANES), BF16),
            pltpu.VMEM((latent_width * heads, LANES), BF16),
            pltpu.VMEM((latent_width * heads, LANES), BF16),
            pltpu.VMEM((max(rows, latent_width) * heads, LANES), F32),
            pltpu.VMEM((heads, rope, rows), BF16),
            pltpu.VMEM((share, width), BF16),
            pltpu.VMEM((heads, rows, wide), BF16),
            pltpu.VMEM((latent_width, heads * LANES), BF16),
            pltpu.VMEM((keys, wide), BF16),
            pltpu.VMEM((width, hh), BF16),
            pltpu.VMEM((n, hh, dblk), BF16),
            pltpu.VMEM(out_weight.shape, BF16),
            pltpu.VMEM((nz, heads * rows, chunk), F32),
            pltpu.VMEM((heads * rows, LANES), F32),
            pltpu.VMEM((rows, latent_width), F32),
            pltpu.VMEM((2, nx * share, out_weight.shape[0]), BF16),
            pltpu.VMEM((nx, share, width), BF16),
            pltpu.VMEM((nx, share, width), BF16),
            pltpu.VMEM((nx, share, width), F32),
            pltpu.VMEM((max(nx - 1, 1), share, width), BF16),
            pltpu.VMEM((max(nx - 1, 1), share, width), BF16),
            pltpu.VMEM((rows, LANES), F32),
            pltpu.VMEM((tp, share, LANES), F32),
            pltpu.VMEM((share, width), F32),
            pltpu.VMEM((2, tp, share, width), BF16),
            pltpu.VMEM((2, rows, hh), BF16),
            pltpu.VMEM((2, nx, share, dblk), F32),
            pltpu.VMEM((n, 2, nx, share, dblk), F32),
            pltpu.VMEM((n, 2, nx, share, dblk), BF16),
            pltpu.VMEM((n, 2, nx, share, dblk), BF16),
            pltpu.VMEM((n, 2, max(nx - 1, 1), share, dblk), BF16),
            pltpu.VMEM((n, 2, max(nx - 1, 1), share, dblk), BF16),
            pltpu.VMEM((n, share, dblk), BF16),
            pltpu.VMEM((n, share, dblk), BF16),
            dma((8,)),
            dma((n,)), dma((n,)), dma((n, nx)), dma((n, nx)), dma((n, nx)), dma((n, nx)),
            dma((2,)), dma((2, hz)),
            dma((2, hz + 1, 2, m)), dma((2, hz + 1, 2, m)),
            dma((tp,)), dma((tp,)), dma((nx,)), dma((nx,)),
            dma((2, 2, nx)), dma((2, 2, nx)),
            dma((n, 2)), dma((n, 2)), dma((n, 2, nx)), dma((n, 2, nx)), dma((n,)), dma((n,)),
        ],
        compiler_params=pltpu.CompilerParams(
            collective_id=0, has_side_effects=True, vmem_limit_bytes=63 * 1024 * 1024
        ),
    )(
        latent, latent_gain[None, :], rope_key.T, jnp.cos(angles), jnp.sin(angles),
        query_nope.reshape(-1, LANES), query_rope.transpose(1, 2, 0),
        key_up.reshape(-1, LANES), value_up.reshape(-1, LANES), out_gain[None, :], out_weight,
        stream, norm_gain[None, :], ff_in, ff_out,
    )


def solution(mesh):
    placed = (
        P(("sp", "tp"), None),
        P("sp", "tp", None),
        P("sp", "tp", None),
        P("sp", None),
        P("sp", None),
        P(),
        P(None, "tp", None),
        P(None, "tp", None),
        P("tp"),
        P("tp", None),
        P(),
        P("sp", "tp"),
        P("tp", "sp"),
    )
    return jax.shard_map(
        functools.partial(body, mesh.shape["sp"], mesh.shape["tp"]),
        mesh=mesh, in_specs=placed, out_specs=P(("sp", "tp"), None), check_vma=False
    )
```

```python
import functools
import math

import jax
import jax.numpy as jnp
from jax import lax
from jax.experimental import pallas as pl
from jax.experimental.pallas import tpu as pltpu
from jax.sharding import PartitionSpec as P

EPS = 1e-06
THETA = 10000.0
F32 = jnp.float32
BF16 = jnp.bfloat16
MESH = pl.DeviceIdType.MESH
LANES = 128


def ring_shape(n):
    rows = 1
    while rows * rows < n:
        rows *= 2
    return (rows, n // rows) if n % rows == 0 else (n, 1)


def ring_pos(nz, ny, index):
    if ny == 1:
        return index
    z, y = lax.div(index, ny), lax.rem(index, ny)
    r = nz - 1 - z
    odd = lax.rem(r, 2)
    c = (1 - odd) * (y - 1) + odd * (ny - 1 - y)
    return jnp.where(y == 0, z, nz + r * (ny - 1) + c)


def ring_at(nz, ny, pos):
    if ny == 1:
        return pos
    q = jnp.maximum(pos - nz, 0)
    r, c = lax.div(q, ny - 1), lax.rem(q, ny - 1)
    odd = lax.rem(r, 2)
    y = 1 + (1 - odd) * c + odd * (ny - 2 - c)
    return jnp.where(pos < nz, pos * ny, (nz - 1 - r) * ny + y)


def flip(index, bits):
    bit = 1
    out = index
    while bit <= bits:
        if bits & bit:
            out = out + bit * (1 - 2 * lax.rem(lax.div(index, bit), 2))
        bit *= 2
    return out


def kernel(
    n, tp, heads, latent_width, width,
    lat_ref, lgain_ref, rk_ref, cos_ref, sin_ref, qn_ref, qr_ref, kup_ref, vup_ref,
    gain_ref, ow_ref, stream_ref, ngain_ref, ffin_ref, ffout_ref,
    out_ref,
    qraw, kraw, vraw, plain, rope_q, base, q, vup, kv, fi, fo, ow, sc, top, acc, gated, pout, pin, keep, xout, xin, sq_out, sq_in, mid, xs, act,
    fresh, mixed, mpo, mpi, mxo, mxi, mzo, mzi,
    local_sem, ka_send, ka_recv, kx_send, kx_recv, kp_send, kp_recv,
    c_send, c_recv, w_send, w_recv,
    s_send, s_recv, r_send, r_recv, g_send, g_recv,
    mp_send, mp_recv, mx_send, mx_recv, mz_send, mz_recv,
):
    sp = lax.axis_index("sp")
    me = lax.axis_index("tp")
    nz, ny = ring_shape(n)
    hz, m, nx = nz // 2, n // 2, tp // 2
    z, y = lax.div(sp, ny), lax.rem(sp, ny)
    x, core = lax.div(me, 2), lax.rem(me, 2)
    half, local = lax.div(sp, m), lax.rem(sp, m)
    zl = lax.div(local, ny)
    mate = lax.rem(sp + m, n)
    pcore = me + 1 - 2 * core
    rows = q.shape[1]
    share = rows // tp
    dblk = width // n
    hh = act.shape[2]
    chunk = sc.shape[2]
    vdim = LANES
    pos = ring_pos(hz, ny, local)

    def at(offset):
        return half * m + ring_at(hz, ny, lax.rem(pos + offset + m, m))

    turnway = lax.rem(pos, 2)

    def space(kz, ky):
        return flip(z, kz) * ny + flip(y, ky)

    def along(kx, c):
        return flip(x, kx) * 2 + c

    sends = []

    def remote(a, b, s, r, to, when=None):
        cp = pltpu.make_async_remote_copy(a, b, s, r, device_id=to, device_id_type=MESH)
        cp.start()
        sends.append(cp)

    def arrived(ref, s, r):
        pltpu.make_async_remote_copy(
            ref, ref, s, r, device_id=(sp, pcore), device_id_type=MESH).wait_recv()

    def lanes(h):
        return pl.ds(pl.multiple_of(h * hh, LANES), hh)

    def deep(h):
        return pl.ds(pl.multiple_of(h * hh, LANES), hh)

    def block_rows(s):
        return pl.ds(pl.multiple_of(s * dblk, dblk), dblk)

    barrier = pltpu.get_barrier_semaphore()
    for i in range(1, n):
        pl.semaphore_signal(
            barrier, inc=1, device_id=(lax.rem(sp + i, n), me), device_id_type=MESH)
    for j in range(1, tp):
        pl.semaphore_signal(
            barrier, inc=1, device_id=(sp, lax.rem(me + j, tp)), device_id_type=MESH)
    own = [
        pltpu.make_async_copy(qn_ref, qraw, local_sem.at[0]),
        pltpu.make_async_copy(ffin_ref.at[:, lanes(half)], fi.at[block_rows(sp)], local_sem.at[1]),
        pltpu.make_async_copy(ffout_ref.at[deep(half)], fo.at[sp], local_sem.at[2]),
        pltpu.make_async_copy(ow_ref, ow, local_sem.at[3]),
        pltpu.make_async_copy(kup_ref, kraw, local_sem.at[4]),
        pltpu.make_async_copy(vup_ref, vraw, local_sem.at[5]),
        pltpu.make_async_copy(qr_ref, rope_q, local_sem.at[6]),
        pltpu.make_async_copy(stream_ref, base, local_sem.at[7]),
    ]
    for c in (1, 2, 0, 4, 6, 5, 3, 7):
        own[c].start()

    rope = rk_ref.shape[0]
    hw = rope // 2

    def turned(values):
        v = values.astype(F32)
        a, b = v[:hw], v[hw:]
        c, s = cos_ref[...], sin_ref[...]
        parts = [a * c - b * s, a * s + b * c]
        if rope % LANES:
            parts.append(jnp.zeros((-rope % LANES, rows), F32))
        return jnp.concatenate(parts, axis=0).T.astype(BF16)

    here = pl.ds(pl.multiple_of(sp * rows, rows), rows)
    full = lat_ref[...].astype(F32)
    spread_out = lax.rsqrt(jnp.mean(full * full, axis=-1, keepdims=True) + EPS)
    kv[here, pl.ds(0, latent_width)] = (full * spread_out * lgain_ref[...]).astype(BF16)
    kv[here, pl.ds(latent_width, kv.shape[1] - latent_width)] = turned(rk_ref[...])

    pl.semaphore_wait(barrier, n + tp - 2)

    def piece(s, t):
        return kv.at[pl.ds(pl.multiple_of(s * rows + t * share, share), share)]

    def arrive(kz, ky):
        ref = piece(space(kz, ky), me)
        i = kz * ny + ky
        arrived(ref, ka_send.at[i], ka_recv.at[i])
        if ky == 0:
            for k in range(1, ny):
                j = kz * ny + k
                remote(ref, ref, ka_send.at[j], ka_recv.at[j], (space(0, k), me))
        for kx in range(1, nx):
            remote(ref, ref, kx_send.at[i, kx], kx_recv.at[i, kx], (sp, along(kx, core)))
        remote(ref, ref, kp_send.at[i, 0], kp_recv.at[i, 0], (sp, pcore))

    def across(kz, ky):
        i = kz * ny + ky
        for kx in range(1, nx):
            ref = piece(space(kz, ky), along(kx, core))
            arrived(ref, kx_send.at[i, kx], kx_recv.at[i, kx])
            remote(ref, ref, kp_send.at[i, kx], kp_recv.at[i, kx], (sp, pcore))

    def settle(kz, ky):
        i = kz * ny + ky
        for kx in range(nx):
            ref = piece(space(kz, ky), along(kx, 1 - core))
            arrived(ref, kp_send.at[i, kx], kp_recv.at[i, kx])

    def inner_of(h):
        return (hz - 1) * (1 - h)

    def is_inner(hm):
        return lax.div(lax.rem(hm, m), ny) == inner_of(half)

    def w_whole(b, s):
        return fi.at[block_rows(s)] if b == 0 else fo.at[s]

    def w_ref(b, s, way):
        if b == 0:
            return fi.at[pl.ds(pl.multiple_of(s * dblk + way * (dblk // 2), dblk // 2), dblk // 2)]
        return fo.at[s, pl.ds(pl.multiple_of(way * (hh // 2), hh // 2), hh // 2)]

    def home(way, step):
        return at((2 * way - 1) * step)

    def source(g, hm):
        if g == 0:
            return hm
        return (1 - half) * m + (g - 1) * ny + lax.rem(hm, ny)

    def cross(b):
        to = (1 - half) * m + inner_of(1 - half) * ny + y
        a = ffin_ref.at[:, lanes(1 - half)] if b == 0 else ffout_ref.at[deep(1 - half)]
        remote(a, w_whole(b, sp), c_send.at[b], c_recv.at[b, zl], (to, me))

    guarded = []

    def unit(b, g, step, k):
        way = turnway if k == 0 else 1 - turnway
        hm = home(way, step)
        s = source(g, hm)
        ref = w_ref(b, s, way)
        if step < m - 1:
            cp = pltpu.make_async_remote_copy(
                ref, ref, w_send.at[b, g, way, step], w_recv.at[b, g, way, step],
                device_id=(at(1 - 2 * way), me), device_id_type=MESH)

        def go():
            if step > 0:
                arrived(ref, w_send.at[b, g, way, step - 1], w_recv.at[b, g, way, step - 1])
            elif g > 0 and k == 0:
                arrived(w_whole(b, s), c_send.at[b], c_recv.at[b, g - 1])
            if step < m - 1:
                cp.start()

        if g == 0:
            go()
            if step < m - 1:
                sends.append(cp)
        else:
            pl.when(is_inner(hm))(go)
            if step < m - 1:
                guarded.append((hm, cp))

    others = range(1, hz + 1)
    issued = set()

    def do(b, g, step, k):
        if step < m and (b, g, step, k) not in issued:
            if step > 0:
                do(b, g, step - 1, k)
            issued.add((b, g, step, k))
            unit(b, g, step, k)

    def near(b, step, *ks):
        for k in ks:
            do(b, 0, step, k)

    def far(b, step, *ks, groups=None):
        for g in groups or others:
            for k in ks:
                do(b, g, step, k)

    mine = piece(sp, me)
    for ky in range(1, ny):
        remote(mine, mine, ka_send.at[ky], ka_recv.at[ky], (space(0, ky), me))
    for kz in range(1, nz):
        remote(mine, mine, ka_send.at[kz * ny], ka_recv.at[kz * ny], (space(kz, 0), me))
    own[1].wait()
    near(0, 0, 0, 1)

    scale = math.log2(math.e) / math.sqrt(LANES + rope)
    strip = 2 * LANES
    team = heads * rows

    def score(kz):
        base = flip(z, kz) * chunk

        def one(t, _):
            keys = pl.ds(pl.multiple_of(base + t * strip, strip), strip)
            s = lax.dot_general(
                q[...].reshape(team, q.shape[2]), kv[keys, :], (((1,), (1,)), ((), ())),
                preferred_element_type=F32) * scale
            sc[kz, :, pl.ds(pl.multiple_of(t * strip, strip), strip)] = s
            best = jnp.maximum(s[:, :LANES], s[:, LANES:])
            top[...] = jnp.maximum(top[...], best)
            return 0

        lax.fori_loop(0, chunk // strip, one, 0)

    top[...] = jnp.full(top.shape, -jnp.inf, F32)

    def unpack(raw, count):
        plain[pl.ds(0, count * heads), :] = raw[...].astype(F32)

    def head_rows(h, count):
        return plain[pl.ds(h, count, stride=heads), :].astype(BF16)

    own[0].wait()
    unpack(qraw, rows)
    for h in range(heads):
        q[h, :, pl.ds(0, vdim)] = head_rows(h, rows)
    own[4].wait()
    unpack(kraw, latent_width)
    for h in range(heads):
        q[h, :, pl.ds(0, latent_width)] = lax.dot_general(
            q[h, :, pl.ds(0, vdim)], head_rows(h, latent_width), (((1,), (1,)), ((), ())),
            preferred_element_type=F32).astype(BF16)
    for ky in range(1, ny):
        arrive(0, ky)
    arrive(1, 0)
    own[6].wait()
    for h in range(heads):
        q[h, :, pl.ds(latent_width, q.shape[2] - latent_width)] = turned(rope_q[h])
    own[5].wait()
    unpack(vraw, latent_width)
    for h in range(heads):
        vup[:, h * vdim:(h + 1) * vdim] = head_rows(h, latent_width)
    for ky in range(1, ny):
        across(0, ky)
    for kz in range(2, nz):
        arrive(kz, 0)
    own[2].wait()
    cross(0)
    near(1, 0, 0, 1)
    for ky in range(1, ny):
        settle(0, ky)
    for ky in range(1, ny):
        arrive(1, ky)
    score(0)
    for kz in range(1, nz):
        for ky in range(1, ny):
            if kz > 1:
                arrive(kz, ky)
    near(0, 1, 0)
    for kz in range(1, nz):
        for ky in range(ny):
            across(kz, ky)
        for ky in range(ny):
            settle(kz, ky)
        score(kz)
        if kz == 1:
            cross(1)
            near(1, 1, 0)
            near(0, 1, 1)
        elif kz == nz - 1:
            near(0, 2, 0)

    squares = jnp.zeros((rows, 1), F32)
    for h in range(heads):
        team_rows = slice(h * rows, (h + 1) * rows)
        peak = jnp.max(top[team_rows], axis=1, keepdims=True)
        acc[...] = jnp.zeros_like(acc)

        def gather(kz, den):
            zk = flip(z, 0)
            zk = jnp.where(kz == 0, z, zk)
            for k in range(1, nz):
                zk = jnp.where(kz == k, flip(z, k), zk)
            e = jnp.exp2(sc[kz, team_rows] - peak)
            acc[...] += jnp.dot(
                e.astype(BF16),
                kv[pl.ds(pl.multiple_of(zk * chunk, chunk), chunk), pl.ds(0, latent_width)],
                preferred_element_type=F32)
            return den + jnp.sum(e, axis=1, keepdims=True)

        den = lax.fori_loop(0, nz, gather, jnp.zeros((rows, 1), F32))
        lat = (acc[...] / den).astype(BF16)
        cols = slice(h * vdim, (h + 1) * vdim)
        one = jnp.dot(lat, vup[:, cols], preferred_element_type=F32)
        squares = squares + jnp.sum(one * one, axis=1, keepdims=True)
        scaled = (one * gain_ref[:, cols]).astype(BF16)
        for t in range(tp):
            gated[t % 2, (t // 2) * share:(t // 2 + 1) * share, cols] = (
                scaled[t * share:(t + 1) * share])
        if h == 0:
            near(1, 1, 1)
        if h == heads // 2 - 1:
            far(0, 0, 0, 1)
        if h == heads // 2:
            near(0, 2, 1)
    sq_out[...] = jnp.broadcast_to(squares, sq_out.shape)
    own[3].wait()

    tile = width // 4

    def project(which, put):
        def one(c, _):
            cols = pl.ds(pl.multiple_of(c * tile, tile), tile)
            got = jnp.dot(gated[which], ow[:, cols], preferred_element_type=F32)
            put(cols, got.reshape(nx, share, tile))
            return 0
        lax.fori_loop(0, 4, one, 0)

    def put_out(cols, got):
        pout[:, :, cols] = got.astype(BF16)

    def put_keep(cols, got):
        keep[:, :, cols] = got

    project(1 - core, put_out)
    remote(pout, pin, r_send.at[0], r_recv.at[0], (sp, pcore))
    for j in range(1, tp):
        to = lax.rem(me + j, tp)
        remote(sq_out.at[pl.ds(pl.multiple_of(to * share, share), share)], sq_in.at[j],
               s_send.at[j], s_recv.at[j], (sp, to))
    project(core, put_keep)
    arrived(pin, r_send.at[0], r_recv.at[0])
    for kx in range(1, nx):
        xi = flip(x, kx)
        xout[kx - 1] = (keep[xi] + pin[xi].astype(F32)).astype(BF16)
        remote(xout.at[kx - 1], xin.at[kx - 1], r_send.at[kx], r_recv.at[kx], (sp, along(kx, core)))
    far(0, 1, 0, 1)
    near(1, 2, 1)
    summed = keep[x] + pin[x].astype(F32)
    square = sq_out[pl.ds(pl.multiple_of(me * share, share), share)]
    for j in range(1, tp):
        arrived(sq_in.at[j], s_send.at[j], s_recv.at[j])
        square = square + sq_in[j]
    for kx in range(1, nx):
        arrived(xin.at[kx - 1], r_send.at[kx], r_recv.at[kx])
        summed = summed + xin[kx - 1].astype(F32)
    row_scale = lax.rsqrt(square[:, :1] / (heads * tp * vdim) + EPS)
    own[7].wait()
    middle = base[...].astype(F32) + row_scale * summed
    mid[...] = middle
    norm = lax.rsqrt(jnp.mean(middle * middle, axis=1, keepdims=True) + EPS)

    def seat(kx, c):
        return c * nx + flip(x, kx)

    xs[0, seat(0, core)] = (middle * norm * ngain_ref[...]).astype(BF16)

    def hand(s, kx):
        ref = xs.at[s, seat(kx, core)]
        remote(ref, ref, g_send.at[1, s, kx], g_recv.at[1, s, kx], (sp, pcore))

    def spread(s):
        ref = xs.at[s, seat(0, core)]
        for kx in range(1, nx):
            remote(ref, ref, g_send.at[0, s, kx], g_recv.at[0, s, kx], (sp, along(kx, core)))
        hand(s, 0)

    def collect(s):
        for kx in range(1, nx):
            arrived(xs.at[s, seat(kx, core)], g_send.at[0, s, kx], g_recv.at[0, s, kx])
            hand(s, kx)

    def settled(s):
        for kx in range(nx):
            arrived(xs.at[s, seat(kx, 1 - core)], g_send.at[1, s, kx], g_recv.at[1, s, kx])

    ref = xs.at[0, seat(0, core)]
    remote(ref, xs.at[1, seat(0, core)], g_send.at[0, 0, 0], g_recv.at[0, 0, 0], (mate, me))
    spread(0)
    far(1, 0, 0, 1)
    far(0, 2, 0, 1)
    near(0, m - 1, 0, 1)
    collect(0)
    settled(0)
    far(1, 1, 0)
    near(1, 2, 0)
    far(0, m - 1, 0, 1)

    wide = 512 if hh % 512 == 0 else 128

    def first(s):
        for c in range(hh // wide):
            cols = slice(c * wide, (c + 1) * wide)
            pre = jnp.dot(
                xs[s].reshape(rows, width), fi[:, cols], preferred_element_type=F32)
            pre = jnp.maximum(pre, 0.0)
            act[s, :, cols] = (pre * pre).astype(BF16)

    flow = []
    for k in range(m):
        flow.append((0, at(k)))
    for g in others:
        for ky in range(ny):
            flow.append((g, (1 - half) * m + (g - 1) * ny + flip(y, ky)))

    def stage_dot(i, u):
        got = jnp.dot(act[u], fo[flow[i][1]], preferred_element_type=F32)
        fresh[...] = got.reshape(2, nx, share, dblk)
        mixed[i, u] = fresh[core]
        mpo[i, u] = fresh[1 - core].astype(BF16)
        remote(mpo.at[i, u], mpi.at[i, u], mp_send.at[i, u], mp_recv.at[i, u], (sp, pcore))

    def stage_core(i, u):
        arrived(mpi.at[i, u], mp_send.at[i, u], mp_recv.at[i, u])
        for kx in range(1, nx):
            xi = flip(x, kx)
            mxo[i, u, kx - 1] = (
                mixed[i, u, xi] + mpi[i, u, xi].astype(F32)).astype(BF16)
            remote(mxo.at[i, u, kx - 1], mxi.at[i, u, kx - 1], mx_send.at[i, u, kx],
                   mx_recv.at[i, u, kx], (sp, along(kx, core)))

    def stage_x(i, u):
        s = flow[i][1]
        v = mixed[i, u, x] + mpi[i, u, x].astype(F32)
        for kx in range(1, nx):
            arrived(mxi.at[i, u, kx - 1], mx_send.at[i, u, kx], mx_recv.at[i, u, kx])
            v = v + mxi[i, u, kx - 1].astype(F32)
        if u == 1:
            mzo[s] = v.astype(BF16)
            remote(mzo.at[s], mzi.at[s], mz_send.at[s], mz_recv.at[s], (mate, me))
        else:
            cols = pl.ds(pl.multiple_of(s * dblk, dblk), dblk)
            mid[:, cols] = mid[:, cols] + v

    to_core, to_x = [], []

    def drain(cores, xs_left):
        while len(to_core) > cores:
            stage_core(*to_core[0])
            to_x.append(to_core.pop(0))
        while len(to_x) > xs_left:
            stage_x(*to_x.pop(0))

    def push(i, u):
        stage_dot(i, u)
        to_core.append((i, u))
        drain(1, 3)

    arrived(xs.at[1, seat(0, core)], g_send.at[0, 0, 0], g_recv.at[0, 0, 0])
    spread(1)
    far(1, 1, 1, groups=others[:1])
    first(0)
    far(1, 1, 1)
    early = [0, 2] if m == 4 else [0]
    late = [i for i in range(m) if i not in early]
    for i in early:
        push(i, 0)
    drain(0, 8)
    collect(1)
    far(1, 2, 0, 1, groups=others[:1])
    settled(1)
    first(1)
    for i in early:
        push(i, 1)
    far(1, 2, 0, 1)
    rest = list(late)
    for g in others:
        mine_g = [i for i in range(m, n) if flow[i][0] == g]
        for k in range(2):
            do(1, g, m - 1, k)
        for i in mine_g:
            push(i, 1)
        if g == 1:
            near(1, m - 1, 0, 1)
            for i in late:
                push(i, 1)
        rest += mine_g
    for i in rest:
        push(i, 0)
    drain(0, 0)
    for i in range(n):
        s = flow[i][1]
        arrived(mzi.at[s], mz_send.at[s], mz_recv.at[s])
        cols = pl.ds(pl.multiple_of(s * dblk, dblk), dblk)
        out_ref[:, cols] = (mid[:, cols] + mzi[s].astype(F32)).astype(BF16)

    for cp in sends:
        cp.wait_send()
    for hm, cp in guarded:
        pl.when(is_inner(hm))(cp.wait_send)


def body(
    n, tp,
    stream, query_nope, query_rope, latent, rope_key, latent_gain,
    key_up, value_up, out_gain, out_weight, norm_gain, ff_in, ff_out,
):
    rows, heads = query_nope.shape[:2]
    width = stream.shape[1]
    latent_width = latent.shape[1]
    rope = rope_key.shape[1]
    dblk, hidden = ff_in.shape
    share = rows // tp
    positions = (lax.axis_index("sp") * rows + jnp.arange(rows, dtype=jnp.int32)).astype(F32)
    inverse = jnp.power(THETA, -jnp.arange(0, rope, 2, dtype=F32) / rope)
    angles = positions[None, :] * inverse[:, None]
    wide = latent_width + rope + (-rope) % LANES
    keys = n * rows
    nz, ny = ring_shape(n)
    hz, m, nx = nz // 2, n // 2, tp // 2
    chunk = ny * rows
    hh = hidden // 2
    vm = pl.BlockSpec(memory_space=pltpu.VMEM)
    hbm = pl.BlockSpec(memory_space=pl.ANY)
    dma = pltpu.SemaphoreType.DMA
    return pl.pallas_call(
        functools.partial(kernel, n, tp, heads, latent_width, width),
        out_shape=jax.ShapeDtypeStruct((share, width), BF16),
        in_specs=[vm, vm, vm, vm, vm, hbm, hbm, hbm, hbm, vm, hbm, hbm, vm, hbm, hbm],
        out_specs=vm,
        scratch_shapes=[
            pltpu.VMEM((rows * heads, LANES), BF16),
            pltpu.VMEM((latent_width * heads, LANES), BF16),
            pltpu.VMEM((latent_width * heads, LANES), BF16),
            pltpu.VMEM((max(rows, latent_width) * heads, LANES), F32),
            pltpu.VMEM((heads, rope, rows), BF16),
            pltpu.VMEM((share, width), BF16),
            pltpu.VMEM((heads, rows, wide), BF16),
            pltpu.VMEM((latent_width, heads * LANES), BF16),
            pltpu.VMEM((keys, wide), BF16),
            pltpu.VMEM((width, hh), BF16),
            pltpu.VMEM((n, hh, dblk), BF16),
            pltpu.VMEM(out_weight.shape, BF16),
            pltpu.VMEM((nz, heads * rows, chunk), F32),
            pltpu.VMEM((heads * rows, LANES), F32),
            pltpu.VMEM((rows, latent_width), F32),
            pltpu.VMEM((2, nx * share, out_weight.shape[0]), BF16),
            pltpu.VMEM((nx, share, width), BF16),
            pltpu.VMEM((nx, share, width), BF16),
            pltpu.VMEM((nx, share, width), F32),
            pltpu.VMEM((max(nx - 1, 1), share, width), BF16),
            pltpu.VMEM((max(nx - 1, 1), share, width), BF16),
            pltpu.VMEM((rows, LANES), F32),
            pltpu.VMEM((tp, share, LANES), F32),
            pltpu.VMEM((share, width), F32),
            pltpu.VMEM((2, tp, share, width), BF16),
            pltpu.VMEM((2, rows, hh), BF16),
            pltpu.VMEM((2, nx, share, dblk), F32),
            pltpu.VMEM((n, 2, nx, share, dblk), F32),
            pltpu.VMEM((n, 2, nx, share, dblk), BF16),
            pltpu.VMEM((n, 2, nx, share, dblk), BF16),
            pltpu.VMEM((n, 2, max(nx - 1, 1), share, dblk), BF16),
            pltpu.VMEM((n, 2, max(nx - 1, 1), share, dblk), BF16),
            pltpu.VMEM((n, share, dblk), BF16),
            pltpu.VMEM((n, share, dblk), BF16),
            dma((8,)),
            dma((n,)), dma((n,)), dma((n, nx)), dma((n, nx)), dma((n, nx)), dma((n, nx)),
            dma((2,)), dma((2, hz)),
            dma((2, hz + 1, 2, m)), dma((2, hz + 1, 2, m)),
            dma((tp,)), dma((tp,)), dma((nx,)), dma((nx,)),
            dma((2, 2, nx)), dma((2, 2, nx)),
            dma((n, 2)), dma((n, 2)), dma((n, 2, nx)), dma((n, 2, nx)), dma((n,)), dma((n,)),
        ],
        compiler_params=pltpu.CompilerParams(
            collective_id=0, has_side_effects=True, vmem_limit_bytes=63 * 1024 * 1024
        ),
    )(
        latent, latent_gain[None, :], rope_key.T, jnp.cos(angles), jnp.sin(angles),
        query_nope.reshape(-1, LANES), query_rope.transpose(1, 2, 0),
        key_up.reshape(-1, LANES), value_up.reshape(-1, LANES), out_gain[None, :], out_weight,
        stream, norm_gain[None, :], ff_in, ff_out,
    )


def solution(mesh):
    placed = (
        P(("sp", "tp"), None),
        P("sp", "tp", None),
        P("sp", "tp", None),
        P("sp", None),
        P("sp", None),
        P(),
        P(None, "tp", None),
        P(None, "tp", None),
        P("tp"),
        P("tp", None),
        P(),
        P("sp", "tp"),
        P("tp", "sp"),
    )
    return jax.shard_map(
        functools.partial(body, mesh.shape["sp"], mesh.shape["tp"]),
        mesh=mesh, in_specs=placed, out_specs=P(("sp", "tp"), None), check_vma=False
    )
```
